32 devices in a mesh: fs: 8 (over z, x), tp: 4 (over y, core).
Axes of the slice: x: 2, y: 2, z: 4, core: 2. Of those that a mesh axis runs over, the one named last changes fastest.
Arguments:
- x_late: bfloat16 [4096, 2048], P(('fs', 'tp')), may hold values from -6 to 6
- x_early: bfloat16 [4096, 2048], P(('fs', 'tp')), may hold values from -6 to 6
- d_hidden: bfloat16 [4096, 3072], P('fs', 'tp'), may hold values from -6 to 6
- w_gate: bfloat16 [2048, 3072], P('fs', 'tp'), may hold values from -0.125 to 0.125
- w_up: bfloat16 [2048, 3072], P('fs', 'tp'), may hold values from -0.125 to 0.125
- gate_sum: float32 [2048, 3072], P('fs', 'tp'), may hold values from -192 to 192
- up_sum: float32 [2048, 3072], P('fs', 'tp'), may hold values from -192 to 192
Outputs:
- hidden_late: bfloat16 [4096, 3072], P('fs', 'tp')
- grad_input: bfloat16 [4096, 2048], P(('fs', 'tp'))
- gate_sum_out: float32 [2048, 3072], P('fs', 'tp')
- up_sum_out: float32 [2048, 3072], P('fs', 'tp')
The draws below stay inside these ranges and needn't reach their ends.
All inputs are finite; a program needn't handle non-finite values.
Results may differ from the reference program's by a relative error of at most 0.0095.
Values may be sent and summed in bfloat16 or wider, within the bound.
A program may use at most 128 MiB of HBM per device.

```python
import jax
import jax.numpy as jnp
from jax import lax

D = 2048
FF = 3072
TOKENS = 4096
N_TP = 4


def with_spikes(result, rng, source, target, shards_of, factor):
    owner, partner = [(jnp.arange(result.shape[dim]) // (result.shape[dim] // shards_of)).reshape([-1 if axis == dim else 1 for axis in range(result.ndim)]) for dim in (source, target)]
    chosen = jax.random.permutation(rng, shards_of)[partner]
    strong = (owner == chosen) | (owner == (partner + shards_of // 2) % shards_of)
    return jnp.where(strong, factor * result, result)


def level_of(stream_key, extent, shards, least, largest):
    factor_of, own = 1.0, jax.random.fold_in(stream_key, 6)
    for axis_at, parts in shards:
        heights = jnp.exp(jax.random.uniform(jax.random.fold_in(own, axis_at), (parts,), jnp.float32, least / len(shards), largest / len(shards)))
        factor_of = factor_of * jnp.repeat(heights, extent[axis_at] // parts).reshape([-1 if axis == axis_at else 1 for axis in range(len(extent))])
    return factor_of


def gaussian(key, extent, spread, limit, shards=(), dtype=jnp.bfloat16):
    gain = level_of(key, extent, shards, -0.22, 0.18) if shards else 1.0
    entries = jax.random.normal(key, extent, jnp.float32) * spread * gain
    return jnp.minimum(jnp.maximum(entries, -limit), limit).astype(dtype)


def gaussian_with(own_key, dims, spread, most, cuts, heavy, held_as=jnp.bfloat16):
    entries = spread * jax.random.normal(own_key, dims, jnp.float32)
    if cuts:
        entries = entries * level_of(own_key, dims, cuts, -0.22, 0.18)
    return jnp.clip(with_spikes(entries, jax.random.fold_in(own_key, 3), *heavy), -most, most).astype(held_as)


def setup_inputs(seed: int = 0) -> dict:
    streams_of = jax.random.split(jax.random.key(seed), 8)
    return {
        "x_late": gaussian(streams_of[0], (TOKENS, D), 1.0, 6.0, ((0, 32),)),
        "x_early": gaussian_with(streams_of[1], (TOKENS, D), 1.0, 6.0, ((0, 32),), (0, 1, 32, 2.75)),
        "d_hidden": gaussian_with(streams_of[2], (TOKENS, FF), 1.0, 6.0, ((0, 8), (1, 4)), (0, 1, 8, 2.0)),
        "w_gate": gaussian(streams_of[3], (D, FF), D ** -0.5, 0.125, ((0, 8), (1, 4))),
        "w_up": gaussian(streams_of[4], (D, FF), D ** -0.5, 0.125, ((0, 8), (1, 4))),
        "gate_sum": gaussian(streams_of[5], (D, FF), (0.5 * TOKENS ** 0.5), 192.0, ((0, 8), (1, 4)), jnp.float32),
        "up_sum": gaussian(streams_of[6], (D, FF), (0.5 * TOKENS ** 0.5), 192.0, ((0, 8), (1, 4)), jnp.float32),
    }


def reference(x_late, x_early, d_hidden, w_gate, w_up, gate_sum, up_sum):
    gate_late = jnp.dot(x_late, w_gate, preferred_element_type=jnp.float32)
    up_late = jnp.dot(x_late, w_up, preferred_element_type=jnp.float32)
    sigmoid_late = jax.nn.sigmoid(gate_late)
    hidden_late = (gate_late * sigmoid_late * up_late).astype(jnp.bfloat16)
    gate_early = jnp.dot(x_early, w_gate, preferred_element_type=jnp.float32)
    up_early = jnp.dot(x_early, w_up, preferred_element_type=jnp.float32)
    sigmoid_early = jax.nn.sigmoid(gate_early)
    cotangent = d_hidden.astype(jnp.float32)
    d_gate = (cotangent * up_early * sigmoid_early * (1.0 + gate_early * (1.0 - sigmoid_early))).astype(jnp.bfloat16)
    d_up = (cotangent * gate_early * sigmoid_early).astype(jnp.bfloat16)
    span = FF // N_TP
    total = jnp.zeros((x_early.shape[0], x_early.shape[1]), jnp.float32)
    for index in range(N_TP):
        lower = index * span
        partial_value = jnp.dot(d_gate[:, lower:lower + span], w_gate[:, lower:lower + span].T, preferred_element_type=jnp.float32)
        partial_value = partial_value + jnp.dot(d_up[:, lower:lower + span], w_up[:, lower:lower + span].T, preferred_element_type=jnp.float32)
        rounded = lax.optimization_barrier(partial_value.astype(jnp.bfloat16))
        total = total + rounded.astype(jnp.float32)
    grad_input = total.astype(jnp.bfloat16)
    gate_sum_out = gate_sum + jnp.dot(x_early.T, d_gate, preferred_element_type=jnp.float32)
    up_sum_out = up_sum + jnp.dot(x_early.T, d_up, preferred_element_type=jnp.float32)
    return (hidden_late, grad_input, gate_sum_out, up_sum_out)
```

```python
import functools

import jax
import jax.numpy as jnp
from jax import lax
from jax.experimental import pallas as pl
from jax.experimental.pallas import tpu as pltpu
from jax.sharding import PartitionSpec as P

MESH = pl.DeviceIdType.MESH
F32 = jnp.float32
BF16 = jnp.bfloat16
LANES = 128


def under(when, action):
    if when is None:
        action()
    else:
        pl.when(when)(action)


class Copies:
    def __init__(self, send_sem, recv_sem):
        self.send_sem, self.recv_sem = send_sem, recv_sem
        self.index, self.sent = {}, []

    def number(self, key):
        return self.index.setdefault(key, len(self.index))

    def make(self, key, src, dst, device):
        at = self.number(key) if isinstance(key, tuple) else key
        return pltpu.make_async_remote_copy(
            src_ref=src, dst_ref=dst, send_sem=self.send_sem.at[at], recv_sem=self.recv_sem.at[at],
            device_id=device, device_id_type=MESH,
        )

    def start(self, key, src, dst, device, when=None):
        copy = self.make(key, src, dst, device)
        self.sent.append((copy, when))
        under(when, copy.start)

    def arrived(self, key, dst, device):
        self.make(key, dst, dst, device).wait_recv()

    def drain(self):
        for copy, when in self.sent:
            under(when, copy.wait_send)


class Locals:
    def __init__(self, sem):
        self.sem, self.copies = sem, {}

    def start(self, key, src, dst):
        copy = pltpu.make_async_copy(src, dst, self.sem.at[len(self.copies)])
        self.copies[key] = [copy, False]
        copy.start()

    def wait(self, key):
        entry = self.copies[key]
        if not entry[1]:
            entry[1] = True
            entry[0].wait()

    def drain(self):
        for key in self.copies:
            self.wait(key)


def flip(index, bit):
    return jnp.where(lax.rem(lax.div(index, bit), 2) == 0, index + bit, index - bit)


def flips(index, mask):
    for bit in (1, 2):
        if mask & bit:
            index = flip(index, bit)
    return index


def aligned(value, size):
    return pl.ds(pl.multiple_of(value, size), size)


NT = (((1,), (1,)), ((), ()))


def layer_kernel(
    fs_count, tp_count, xl, xe, dh, wg, wu, gs, us, hid, gx, og, ou,
    w, ws, te, tl, tt, ct, db, dw, rs, last, dxa, dxb, xk, xq, hm, hs, g, fb, fr, gxv, ssem, rsem, lsem,
):
    fs, tp = lax.axis_index("fs"), lax.axis_index("tp")
    z, x = lax.div(fs, 2), lax.rem(fs, 2)
    n = fs_count // 2
    rows, cols = wg.shape
    tokens, width = xe.shape
    half = cols // 2
    chunks = half // LANES
    pair = 2 * LANES
    up = (jnp.minimum(z + 1, n - 1) * 2 + x, tp)
    down = (jnp.maximum(z - 1, 0) * 2 + x, tp)
    beside = (z * 2 + 1 - x, tp)
    across = (fs, flip(tp, 2))
    core = (fs, flip(tp, 1))
    far = {"core": core, "across": across, "beside": beside}
    copies, local = Copies(ssem, rsem), Locals(lsem)

    def cc(c):
        return pl.ds(c * pair, pair)

    def wrows(at, side):
        return aligned((at * 2 + side) * rows, rows)

    def slot(r):
        return pl.ds(r * tokens, tokens)

    for c in range(chunks):
        for name, src, at in (("g", wg, 0), ("u", wu, LANES)):
            lane = pl.ds(c * pair + at, LANES)
            local.start(("w", c, name), src.at[:, aligned(x * half + c * LANES, LANES)], w.at[wrows(z, x), lane])
            local.start(("ws", c, name), src.at[:, aligned((1 - x) * half + c * LANES, LANES)], ws.at[:, lane])
        if c == 0:
            local.start("te", xe, te.at[slot(0)])
    local.start("tl", xl, tl.at[slot(0)])
    for m in range(tp_count):
        src = dh.at[aligned(flips(tp, m) * tokens, tokens), pl.ds(pl.multiple_of(x * half, LANES), half)]
        local.start(("ct", m), src, ct.at[slot(m)])
    for side in range(2):
        lane = pl.ds(pl.multiple_of((x if side == 0 else 1 - x) * half, LANES), half)
        for which, src in enumerate((gs, us)):
            local.start(("g", which, side), src.at[:, lane], g.at[which, side])

    barrier = pltpu.get_barrier_semaphore()

    def greet(device):
        pl.semaphore_signal(barrier, inc=1, device_id=device, device_id_type=MESH)

    pl.when(z < n - 1)(lambda: greet(up))
    pl.when(z > 0)(lambda: greet(down))
    for device in far.values():
        greet(device)
    ends = jnp.where(z < n - 1, 1, 0) + jnp.where(z > 0, 1, 0)
    pl.semaphore_wait(barrier, len(far) + ends)

    plan = []

    def at(time, action, *args):
        plan.append((time, len(plan), functools.partial(action, *args)))

    ways = (("u", up, z < n - 1), ("d", down, z > 0))

    def own_first(c):
        local.wait(("w", c, "g"))
        local.wait(("w", c, "u"))
        ref = w.at[wrows(z, x), cc(c)]
        for name, device, when in ways:
            copies.start(("w", c, name, 0, 0), ref, ref, device, when)

    def swap_weights(c):
        local.wait(("ws", c, "g"))
        local.wait(("ws", c, "u"))
        copies.start(("b", c), ws.at[:, cc(c)], w.at[wrows(z, x), cc(c)], beside)

    def own_second(c):
        ref = w.at[wrows(z, 1 - x), cc(c)]
        copies.arrived(("b", c), ref, beside)
        for name, device, when in ways:
            copies.start(("w", c, name, 0, 1), ref, ref, device, when)

    def pass_weights(c, step, side):
        for name, device, when in ways:
            origin = z - 1 - step if name == "u" else z + 1 + step
            has = origin >= 0 if name == "u" else origin <= n - 1
            ref = w.at[wrows(jnp.clip(origin, 0, n - 1), x if side == 0 else 1 - x), cc(c)]
            pl.when(has)(lambda: copies.arrived(("w", c, name, step, side), ref, device))
            if step < n - 2:
                copies.start(("w", c, name, step + 1, side), ref, ref, device, has & when)

    arrays = {"e": (te, xe, "te"), "l": (tl, xl, "tl")}

    def send_block(kind, to, src, dst, part=None):
        buf = arrays[kind][0]
        if part is None:
            a, b = slot(src), slot(dst)
        else:
            a, b = (pl.ds(r * tokens + part * (tokens // 2), tokens // 2) for r in (src, dst))
        copies.start((kind, to, dst, part), buf.at[a], buf.at[b], far[to])

    def got_block(kind, to, dst, part=None):
        buf = arrays[kind][0]
        a = slot(dst) if part is None else pl.ds(dst * tokens + part * (tokens // 2), tokens // 2)
        copies.arrived((kind, to, dst, part), buf.at[a], far[to])

    def own_block(kind, to):
        local.wait(arrays[kind][2])
        send_block(kind, to, 0, {"core": 1, "across": 2, "beside": 4}[to])

    def from_core(kind):
        got_block(kind, "core", 1)

    def from_across(kind):
        got_block(kind, "across", 2)
        send_block(kind, "beside", 2, 6, 1)
        send_block(kind, "core", 2, 3)

    def from_beside(kind):
        got_block(kind, "beside", 4)
        send_block(kind, "across", 4, 6, 0)
        send_block(kind, "core", 4, 5)

    def from_diagonal(kind):
        got_block(kind, "across", 6, 0)
        got_block(kind, "beside", 6, 1)
        send_block(kind, "core", 6, 7)

    def rest_blocks(kind):
        for r in (3, 5, 7):
            got_block(kind, "core", r)

    def turn(*blocks):
        for r in blocks:
            tt[:, slot(r)] = te[slot(r), :].T

    def swap_cotangent():
        for m in range(tp_count):
            src = dh.at[aligned(flips(tp, m) * tokens, tokens), pl.ds(pl.multiple_of((1 - x) * half, LANES), half)]
            copies.start(("c", m), src, ct.at[slot(tp_count + m)], beside)

    def got_cotangent():
        for m in range(tp_count):
            local.wait(("ct", m))
            copies.arrived(("c", m), ct.at[slot(tp_count + m)], beside)

    tile = 2 * tokens
    tiles = 2 * tp_count * tokens // tile

    def early(c):
        def body(i, carry):
            at_rows = aligned(i * tile, tile)
            pre = jnp.dot(te[at_rows, :], w[:, cc(c)], preferred_element_type=F32)
            gate, up_part = pre[:, :LANES], pre[:, LANES:]
            s = jax.nn.sigmoid(gate)
            cot = ct[at_rows, pl.ds(c * LANES, LANES)].astype(F32)
            db[at_rows, pl.ds(c * pair, LANES)] = (cot * up_part * s * (1.0 + gate * (1.0 - s))).astype(BF16)
            db[at_rows, pl.ds(c * pair + LANES, LANES)] = (cot * gate * s).astype(BF16)
            return carry

        lax.fori_loop(0, tiles, body, 0)

    def late(c):
        def body(first, out, i, carry):
            at_rows = aligned(i * tile, tile)
            from_rows = aligned(first * tp_count * tokens + i * tile, tile)
            pre = jnp.dot(tl[from_rows, :], w[:, cc(c)], preferred_element_type=F32)
            gate, up_part = pre[:, :LANES], pre[:, LANES:]
            out[at_rows, pl.ds(c * LANES, LANES)] = (gate * jax.nn.sigmoid(gate) * up_part).astype(BF16)
            return carry

        lane = aligned(x * half + c * LANES, LANES)
        for first, buf in ((1, hs), (0, hm)):
            lax.fori_loop(0, tiles // 2, functools.partial(body, first, buf), 0)
            for m in range(tp_count):
                src = buf.at[slot(m), pl.ds(c * LANES, LANES)]
                dst = hid.at[aligned(flips(tp, m) * tokens, tokens), lane]
                if first:
                    copies.start(("h", c, m), src, dst, beside)
                else:
                    local.start(("h", c, m), src, dst)

    def got_hidden():
        lane = pl.ds(pl.multiple_of((1 - x) * half, LANES), LANES)
        for c in range(chunks):
            for m in range(tp_count):
                copies.arrived(("h", c, m), hid.at[pl.ds(0, tokens), lane], beside)

    for c in range(chunks):
        for d in range(2):
            for target in range(n):
                copies.number(("r", c, d, target))

    def trows(target):
        return aligned(target * 2 * rows, 2 * rows)

    def weight_grads(c):
        base = [copies.index["r", c, d, 0] for d in range(2)]
        for i in range(n):
            target = jnp.where(z < n // 2, n - 1 - i, i)
            own = dw.at[trows(target), cc(c)]
            own[...] = jnp.dot(tt[trows(target), :], db[:, cc(c)], preferred_element_type=F32).astype(BF16)
            for d, device, edge in ((0, up, z == 0), (1, down, z == n - 1)):
                when = edge & ((target > z) if d == 0 else (target < z))
                copies.start(base[d] + target, own, rs.at[d, trows(target), cc(c)], device, when)

    def add(a, b):
        return (a.astype(F32) + b.astype(F32)).astype(BF16)

    def pass_sums(c, step, near):
        for low in (True, False):
            d = 0 if low == near else 1
            target = n - 1 - step if d == 0 else step
            mine = (z < n // 2) if low else (z >= n // 2)
            passes = mine & ((target > z) & (z > 0) if d == 0 else (target < z) & (z < n - 1))
            device = up if d == 0 else down
            ref = rs.at[d, pl.ds(target * 2 * rows, 2 * rows), cc(c)]
            own = dw.at[pl.ds(target * 2 * rows, 2 * rows), cc(c)]

            def action():
                copies.arrived(("r", c, d, target), ref, device)
                ref[...] = add(ref[...], own[...])

            pl.when(passes)(action)
            copies.start(("r", c, d, target), ref, ref, device, passes)

    theirs = pl.ds(pl.multiple_of((1 - x) * rows, rows), rows)
    ours = pl.ds(pl.multiple_of(x * rows, rows), rows)

    def settle(c):
        last[...] = dw[trows(z), cc(c)].astype(F32)
        for d, behind in ((0, z > 0), (1, z < n - 1)):
            def take():
                ref = rs.at[d, trows(z), cc(c)]
                copies.arrived(copies.index["r", c, d, 0] + z, ref, beside)
                last[...] = last[...] + ref[...].astype(F32)

            pl.when(behind)(take)
        fb[c] = last[theirs, :].astype(BF16)
        copies.start(("f", c), fb.at[c], fr.at[c], beside)
        lane = pl.ds(c * LANES, LANES)
        for which in range(2):
            local.wait(("g", which, 0))
            g[which, 0, :, lane] = g[which, 0, :, lane] + last[ours, pl.ds(which * LANES, LANES)]

    def finish(c):
        copies.arrived(("f", c), fr.at[c], beside)
        lane = pl.ds(c * LANES, LANES)
        for which in range(2):
            local.wait(("g", which, 1))
            g[which, 1, :, lane] = g[which, 1, :, lane] + fr[c, :, pl.ds(which * LANES, LANES)].astype(F32)

    def write_sums():
        for which, out in enumerate((og, ou)):
            for side in range(2):
                lane = pl.ds(pl.multiple_of((x if side == 0 else 1 - x) * half, LANES), half)
                local.start(("o", which, side), g.at[which, side], out.at[:, lane])

    depth = (chunks - 1) * pair
    bands = [pl.ds(i * (width // 4), width // 4) for i in range(4)]

    def input_grads():
        def body(i, carry):
            at_rows = aligned(i * tile, tile)
            for band in bands:
                dxa[at_rows, band] = lax.dot_general(
                    db[at_rows, pl.ds(0, depth)], w[band, pl.ds(0, depth)], NT, preferred_element_type=F32)
            return carry

        lax.fori_loop(0, tiles, body, 0)

    end = pl.ds(depth, pair)

    def input_pair(q):
        at_rows = pl.ds(q * tile, tile)
        for band in bands:
            value = lax.dot_general(db[at_rows, end], w[band, end], NT, preferred_element_type=F32)
            dxb[at_rows, band] = (dxa[at_rows, band] + value).astype(BF16)
        copies.start(("k", q), dxb.at[slot(2 * q + 1)], xk.at[q], core)

    left, right = pl.ds(0, width // 2), pl.ds(width // 2, width // 2)
    routes = {
        3: (("y", 0, left, across), ("x", 2, right, beside)),
        1: (("y", 1, left, across),),
        2: (("x", 3, right, beside),),
        0: (),
    }

    def core_sum(q):
        copies.arrived(("k", q), xk.at[q], core)
        xk[q] = add(xk[q], dxb[slot(2 * q), :])
        for name, place, part, device in routes[q]:
            copies.start(("q", place), xk.at[q, :, part], xq.at[place], device)

    def turn_corner(place, q, part, to, device, back):
        copies.arrived(("q", place), xq.at[place], back)
        xq[place] = add(xq[place], xk[q, :, part])
        copies.start(("q", to), xq.at[place], xq.at[to], device)

    def finish_input():
        for places, part in (((1, 4), left), ((3, 5), right)):
            total = xk[0, :, part].astype(F32)
            for place in places:
                copies.arrived(("q", place), xq.at[place], core)
                total = total + xq[place].astype(F32)
            gxv[:, part] = total.astype(BF16)
        local.start("gx", gxv, gx)

    span = 2.8 * 2 * (n - 1)
    at(0.0, own_first, 0)
    at(0.1, swap_weights, 0)
    for i, to in enumerate(("core", "across", "beside")):
        at(0.2, own_block, "e", to)
    for c in range(1, chunks):
        at((c - 1) * span + 0.5, own_first, c)
        at((c - 1) * span + 0.6, swap_weights, c)
    for c in range(chunks):
        at(c * span + (1.0 if c else 4.5), own_second, c)
        for step in range(n - 1):
            for side in range(2):
                at(c * span + 5 + (2 * step + side) * 3.2, pass_weights, c, step, side)
    at(5.5, from_core, "e")
    at(5.6, turn, 0, 1)
    at(13.0, from_across, "e")
    at(13.1, swap_cotangent)
    at(16.5, from_beside, "e")
    for to in ("core", "across", "beside"):
        at(17.0, own_block, "l", to)
    at(19.1, turn, 2, 4)
    at(24.0, from_diagonal, "e")
    at(24.1, turn, 6)
    at(24.2, rest_blocks, "e")
    at(24.3, turn, 3, 5, 7)
    at(24.4, got_cotangent)
    at(36.0, from_core, "l")
    at(36.1, from_across, "l")
    at(47.0, from_beside, "l")
    at(51.5, from_diagonal, "l")
    at(52.0, rest_blocks, "l")
    ready = span + 9.0
    for c in range(chunks):
        start = ready + c * span
        at(start, early, c)
        at(start + 2.0, weight_grads, c)
        for step in range(n - 1):
            at(start + 11.0 + step * 5.6, pass_sums, c, step, True)
            at(start + 19.0 + step * 5.6, pass_sums, c, step, False)
        at(start + 19.0 + 5.6 * (n - 2), settle, c)
        at(start + 22.0 + 5.6 * (n - 2), finish, c)
    tail = ready + (chunks - 1) * span
    at(tail - span + 4.0, input_grads)
    for c in range(chunks):
        at(max(tail - 5.0 + c * 2.0, 52.1) if c < chunks - 1 else max(tail + 6.0, 52.2), late, c)
    for i, q in enumerate((3, 1, 2, 0)):
        at(tail + 4.0 + i * 0.3, input_pair, q)
        at(tail + 4.4 + i * 0.3, core_sum, q)
    at(tail + 13.0, turn_corner, 0, 2, left, 4, beside, across)
    at(tail + 13.1, turn_corner, 2, 1, right, 5, across, beside)
    at(tail + 24.5, finish_input)
    for _, _, action in sorted(plan, key=lambda entry: entry[:2]):
        action()
    write_sums()
    got_hidden()
    copies.drain()
    local.drain()
    assert len(copies.index) <= ssem.shape[0] and len(local.copies) <= lsem.shape[0]


def local_part(fs_count, tp_count, x_late, x_early, d_hidden, w_gate, w_up, gate_sum, up_sum):
    n = fs_count // 2
    tokens, width = x_early.shape
    rows, cols = w_gate.shape
    half = cols // 2
    chunks = half // LANES
    group = tp_count * tokens
    pair = 2 * LANES
    hidden_spec = jax.ShapeDtypeStruct((group, cols), BF16)
    remote = chunks * (4 * (n - 1) + 1 + 2 * n + tp_count + 1) + 2 * 9 + tp_count + 10
    locals_count = 4 * chunks + 2 + tp_count + 4 + chunks * tp_count + 5
    any_spec = pl.BlockSpec(memory_space=pl.ANY)
    return pl.pallas_call(
        functools.partial(layer_kernel, fs_count, tp_count),
        out_shape=(
            hidden_spec,
            jax.ShapeDtypeStruct(x_early.shape, BF16),
            jax.ShapeDtypeStruct(gate_sum.shape, F32),
            jax.ShapeDtypeStruct(up_sum.shape, F32),
        ),
        in_specs=[any_spec] * 7,
        out_specs=(any_spec,) * 4,
        scratch_shapes=[
            pltpu.VMEM((width, 2 * half), BF16),
            pltpu.VMEM((rows, 2 * half), BF16),
            pltpu.VMEM((2 * group, width), BF16),
            pltpu.VMEM((2 * group, width), BF16),
            pltpu.VMEM((width, 2 * group), BF16),
            pltpu.VMEM((2 * group, half), BF16),
            pltpu.VMEM((2 * group, 2 * half), BF16),
            pltpu.VMEM((width, 2 * half), BF16),
            pltpu.VMEM((2, width, 2 * half), BF16),
            pltpu.VMEM((2 * rows, pair), F32),
            pltpu.VMEM((2 * group, width), F32),
            pltpu.VMEM((2 * group, width), BF16),
            pltpu.VMEM((tp_count, tokens, width), BF16),
            pltpu.VMEM((6, tokens, width // 2), BF16),
            pltpu.VMEM((group, half), BF16),
            pltpu.VMEM((group, half), BF16),
            pltpu.VMEM((2, 2, rows, half), F32),
            pltpu.VMEM((chunks, rows, pair), BF16),
            pltpu.VMEM((chunks, rows, pair), BF16),
            pltpu.VMEM((tokens, width), BF16),
            pltpu.SemaphoreType.DMA((remote,)),
            pltpu.SemaphoreType.DMA((remote,)),
            pltpu.SemaphoreType.DMA((locals_count,)),
        ],
        compiler_params=pltpu.CompilerParams(
            collective_id=0, has_side_effects=True, vmem_limit_bytes=62 * 1024 * 1024),
        name="layer",
    )(x_late, x_early, d_hidden, w_gate, w_up, gate_sum, up_sum)


def solution(mesh):
    return jax.shard_map(
        functools.partial(local_part, mesh.shape["fs"], mesh.shape["tp"]),
        mesh=mesh,
        in_specs=(
            P(("fs", "tp"), None),
            P(("fs", "tp"), None),
            P("fs", "tp"),
            P("fs", "tp"),
            P("fs", "tp"),
            P("fs", "tp"),
            P("fs", "tp"),
        ),
        out_specs=(P("fs", "tp"), P(("fs", "tp"), None), P("fs", "tp"), P("fs", "tp")),
        check_vma=False,
    )
```

```python
import functools

import jax
import jax.numpy as jnp
from jax import lax
from jax.experimental import pallas as pl
from jax.experimental.pallas import tpu as pltpu
from jax.sharding import PartitionSpec as P

MESH = pl.DeviceIdType.MESH
F32 = jnp.float32
BF16 = jnp.bfloat16
LANES = 128


def under(when, action):
    if when is None:
        action()
    else:
        pl.when(when)(action)


class Copies:
    def __init__(self, send_sem, recv_sem):
        self.send_sem, self.recv_sem = send_sem, recv_sem
        self.index, self.sent = {}, []

    def number(self, key):
        return self.index.setdefault(key, len(self.index))

    def make(self, key, src, dst, device):
        at = self.number(key) if isinstance(key, tuple) else key
        return pltpu.make_async_remote_copy(
            src_ref=src, dst_ref=dst, send_sem=self.send_sem.at[at], recv_sem=self.recv_sem.at[at],
            device_id=device, device_id_type=MESH,
        )

    def start(self, key, src, dst, device, when=None):
        copy = self.make(key, src, dst, device)
        self.sent.append((copy, when))
        under(when, copy.start)

    def arrived(self, key, dst, device):
        self.make(key, dst, dst, device).wait_recv()

    def drain(self):
        for copy, when in self.sent:
            under(when, copy.wait_send)


class Locals:
    def __init__(self, sem):
        self.sem, self.copies = sem, {}

    def start(self, key, src, dst):
        copy = pltpu.make_async_copy(src, dst, self.sem.at[len(self.copies)])
        self.copies[key] = [copy, False]
        copy.start()

    def wait(self, key):
        entry = self.copies[key]
        if not entry[1]:
            entry[1] = True
            entry[0].wait()

    def drain(self):
        for key in self.copies:
            self.wait(key)


def flip(index, bit):
    return jnp.where(lax.rem(lax.div(index, bit), 2) == 0, index + bit, index - bit)


def flips(index, mask):
    for bit in (1, 2):
        if mask & bit:
            index = flip(index, bit)
    return index


def aligned(value, size):
    return pl.ds(pl.multiple_of(value, size), size)


NT = (((1,), (1,)), ((), ()))


def layer_kernel(
    fs_count, tp_count, xl, xe, dh, wg, wu, gs, us, hm, hr, gx, g,
    w, ws, te, tl, tt, ct, db, dw, rs, dxa, dxb, xk, xq, hs, fb, fr, ssem, rsem, lsem,
):
    fs, tp = lax.axis_index("fs"), lax.axis_index("tp")
    z, x = lax.div(fs, 2), lax.rem(fs, 2)
    n = fs_count // 2
    rows, cols = wg.shape
    tokens, width = xe.shape
    half = cols // 2
    chunks = half // LANES
    pair = 2 * LANES
    up = (jnp.minimum(z + 1, n - 1) * 2 + x, tp)
    down = (jnp.maximum(z - 1, 0) * 2 + x, tp)
    beside = (z * 2 + 1 - x, tp)
    across = (fs, flip(tp, 2))
    core = (fs, flip(tp, 1))
    far = {"core": core, "across": across, "beside": beside}
    copies, local = Copies(ssem, rsem), Locals(lsem)

    def cc(c):
        return pl.ds(c * pair, pair)

    def wrows(at, side):
        return aligned((at * 2 + side) * rows, rows)

    def slot(r):
        return pl.ds(r * tokens, tokens)

    for c in range(chunks):
        for name, src, at in (("g", wg, 0), ("u", wu, LANES)):
            lane = pl.ds(c * pair + at, LANES)
            local.start(("w", c, name), src.at[:, aligned(x * half + c * LANES, LANES)], w.at[wrows(z, x), lane])
            local.start(("ws", c, name), src.at[:, aligned((1 - x) * half + c * LANES, LANES)], ws.at[:, lane])
        if c == 0:
            local.start("te", xe, te.at[slot(0)])
    local.start("tl", xl, tl.at[slot(0)])
    for m in range(tp_count):
        src = dh.at[aligned(flips(tp, m) * tokens, tokens), pl.ds(pl.multiple_of(x * half, LANES), half)]
        local.start(("ct", m), src, ct.at[slot(m)])
    for side in range(2):
        lane = pl.ds(pl.multiple_of((x if side == 0 else 1 - x) * half, LANES), half)
        for which, src in enumerate((gs, us)):
            local.start(("g", which, side), src.at[:, lane], g.at[which, side])

    barrier = pltpu.get_barrier_semaphore()

    def greet(device):
        pl.semaphore_signal(barrier, inc=1, device_id=device, device_id_type=MESH)

    pl.when(z < n - 1)(lambda: greet(up))
    pl.when(z > 0)(lambda: greet(down))
    for device in far.values():
        greet(device)
    ends = jnp.where(z < n - 1, 1, 0) + jnp.where(z > 0, 1, 0)
    pl.semaphore_wait(barrier, len(far) + ends)

    plan = []

    def at(time, action, *args):
        plan.append((time, len(plan), functools.partial(action, *args)))

    ways = (("u", up, z < n - 1), ("d", down, z > 0))

    def own_first(c):
        local.wait(("w", c, "g"))
        local.wait(("w", c, "u"))
        ref = w.at[wrows(z, x), cc(c)]
        for name, device, when in ways:
            copies.start(("w", c, name, 0, 0), ref, ref, device, when)

    def swap_weights(c):
        local.wait(("ws", c, "g"))
        local.wait(("ws", c, "u"))
        copies.start(("b", c), ws.at[:, cc(c)], w.at[wrows(z, x), cc(c)], beside)

    def own_second(c):
        ref = w.at[wrows(z, 1 - x), cc(c)]
        copies.arrived(("b", c), ref, beside)
        for name, device, when in ways:
            copies.start(("w", c, name, 0, 1), ref, ref, device, when)

    def weight_piece(c, step, side, name):
        origin = z - 1 - step if name == "u" else z + 1 + step
        has = origin >= 0 if name == "u" else origin <= n - 1
        return w.at[wrows(jnp.clip(origin, 0, n - 1), x if side == 0 else 1 - x), cc(c)], has

    def pass_weights(c, step, side):
        if step == n - 2:
            return
        for name, device, when in ways:
            ref, has = weight_piece(c, step, side, name)
            pl.when(has & when)(lambda: copies.arrived(("w", c, name, step, side), ref, device))
            copies.start(("w", c, name, step + 1, side), ref, ref, device, has & when)

    def collect(c):
        for step in range(n - 1):
            for side in range(2):
                for name, device, when in ways:
                    ref, has = weight_piece(c, step, side, name)
                    if step < n - 2:
                        has = has & jnp.logical_not(when)
                    pl.when(has)(lambda: copies.arrived(("w", c, name, step, side), ref, device))

    arrays = {"e": (te, xe, "te"), "l": (tl, xl, "tl")}

    def block(kind, r, part):
        first, size = (0, tokens) if part is None else part
        return arrays[kind][0].at[pl.ds(r * tokens + first, size)]

    def send_block(kind, to, src, dst, part=None):
        copies.start((kind, to, dst, part), block(kind, src, part), block(kind, dst, part), far[to])

    def got_block(kind, to, dst, part=None):
        copies.arrived((kind, to, dst, part), block(kind, dst, part), far[to])

    middle = tokens // 2
    halves = ((0, middle), (middle, middle))
    side_way = {"e": tokens // 8, "l": middle}
    last_part = {kind: (tokens - size, size) for kind, size in side_way.items()}
    corner = {"e": (halves[0], (middle, middle - side_way["e"])), "l": (halves[0],)}

    def own_block(kind, to):
        local.wait(arrays[kind][2])
        dst = {"core": 1, "across": 2, "beside": 4}[to]
        for part in halves if to == "beside" else (None,):
            send_block(kind, to, 0, dst, part)

    def from_core(kind):
        got_block(kind, "core", 1)

    def from_across(kind):
        got_block(kind, "across", 2)
        send_block(kind, "beside", 2, 6, last_part[kind])
        send_block(kind, "core", 2, 3)

    def from_beside(kind, half_at):
        got_block(kind, "beside", 4, halves[half_at])
        if half_at < len(corner[kind]):
            send_block(kind, "across", 4, 6, corner[kind][half_at])
        send_block(kind, "core", 4, 5, halves[half_at])

    def from_diagonal(kind):
        for part in corner[kind]:
            got_block(kind, "across", 6, part)
        got_block(kind, "beside", 6, last_part[kind])
        send_block(kind, "core", 6, 7)

    def third_block(kind):
        got_block(kind, "core", 3)

    def rest_blocks(kind):
        for part in halves:
            got_block(kind, "core", 5, part)
        got_block(kind, "core", 7)

    def turn(*blocks):
        for r in blocks:
            tt[:, slot(r)] = te[slot(r), :].T

    def swap_cotangent(c):
        lane = aligned((1 - x) * half + c * LANES, LANES)
        for m in range(tp_count):
            src = dh.at[aligned(flips(tp, m) * tokens, tokens), lane]
            dst = ct.at[slot(tp_count + m), pl.ds(c * LANES, LANES)]
            copies.start(("c", c, m), src, dst, beside)

    def got_cotangent(c):
        for m in range(tp_count):
            local.wait(("ct", m))
            copies.arrived(("c", c, m), ct.at[slot(tp_count + m), pl.ds(c * LANES, LANES)], beside)

    tile = 2 * tokens
    tiles = 2 * tp_count * tokens // tile

    def early(c):
        def body(i, carry):
            at_rows = aligned(i * tile, tile)
            pre = jnp.dot(te[at_rows, :], w[:, cc(c)], preferred_element_type=F32)
            gate, up_part = pre[:, :LANES], pre[:, LANES:]
            s = jax.nn.sigmoid(gate)
            cot = ct[at_rows, pl.ds(c * LANES, LANES)].astype(F32)
            db[at_rows, pl.ds(c * pair, LANES)] = (cot * up_part * s * (1.0 + gate * (1.0 - s))).astype(BF16)
            db[at_rows, pl.ds(c * pair + LANES, LANES)] = (cot * gate * s).astype(BF16)
            return carry

        lax.fori_loop(0, tiles, body, 0)

    def late(c, first):
        out = hs if first else hm
        lane = pl.ds(c * LANES, LANES)

        def body(i, carry):
            at_rows = aligned(i * tile, tile)
            from_rows = aligned(first * tp_count * tokens + i * tile, tile)
            pre = jnp.dot(tl[from_rows, :], w[:, cc(c)], preferred_element_type=F32)
            gate, up_part = pre[:, :LANES], pre[:, LANES:]
            out[at_rows, lane] = (gate * jax.nn.sigmoid(gate) * up_part).astype(BF16)
            return carry

        lax.fori_loop(0, tiles // 2, body, 0)
        if first:
            copies.start(("h", c), hs.at[:, lane], hr.at[:, lane], beside)

    def got_hidden():
        for c in range(chunks):
            copies.arrived(("h", c), hr.at[:, pl.ds(c * LANES, LANES)], beside)

    for c in range(chunks):
        for d in range(2):
            for side in range(2):
                for target in range(n):
                    copies.number(("r", c, d, side, target))

    def srows(target, side):
        return wrows(target, x if side == 0 else 1 - x)

    def trows(target):
        return aligned(target * 2 * rows, 2 * rows)

    def weight_grads(c, i):
        target = jnp.where(z < n // 2, n - 1 - i, i)
        own = dw.at[trows(target), cc(c)]
        own[...] = jnp.dot(tt[trows(target), :], db[:, cc(c)], preferred_element_type=F32).astype(BF16)
        for side in (1, 0):
            for d, device, edge in ((0, up, z == 0), (1, down, z == n - 1)):
                when = edge & ((target > z) if d == 0 else (target < z))
                base = copies.index["r", c, d, side, 0]
                piece = dw.at[srows(target, side), cc(c)]
                copies.start(base + target, piece, rs.at[d, srows(target, side), cc(c)], device, when)

    def add(a, b):
        return (a.astype(F32) + b.astype(F32)).astype(BF16)

    def pass_sums(c, step, side, near):
        for low in (True, False):
            d = 0 if low == near else 1
            target = n - 1 - step if d == 0 else step
            mine = (z < n // 2) if low else (z >= n // 2)
            passes = mine & ((target > z) & (z > 0) if d == 0 else (target < z) & (z < n - 1))
            device = up if d == 0 else down
            ref = rs.at[d, srows(target, side), cc(c)]
            own = dw.at[srows(target, side), cc(c)]

            def action():
                copies.arrived(("r", c, d, side, target), ref, device)
                ref[...] = add(ref[...], own[...])

            pl.when(passes)(action)
            copies.start(("r", c, d, side, target), ref, ref, device, passes)

    def settle(c, side):
        rows_here = srows(z, side)
        for d, behind in ((0, z > 0), (1, z < n - 1)):
            ref = rs.at[d, rows_here, cc(c)]

            def take():
                copies.arrived(copies.index["r", c, d, side, 0] + z, ref, beside)

            def blank():
                ref[...] = jnp.zeros((rows, pair), BF16)

            pl.when(behind)(take)
            pl.when(jnp.logical_not(behind))(blank)
        total = dw[rows_here, cc(c)].astype(F32)
        for d in range(2):
            total = total + rs[d, rows_here, cc(c)].astype(F32)
        if side == 1:
            fb[c] = total.astype(BF16)
            copies.start(("f", c), fb.at[c], fr.at[c], beside)
            return
        lane = pl.ds(c * LANES, LANES)
        for which in range(2):
            local.wait(("g", which, 0))
            g[which, 0, :, lane] = g[which, 0, :, lane] + total[:, which * LANES : (which + 1) * LANES]

    def finish(c):
        copies.arrived(("f", c), fr.at[c], beside)
        lane = pl.ds(c * LANES, LANES)
        for which in range(2):
            local.wait(("g", which, 1))
            g[which, 1, :, lane] = g[which, 1, :, lane] + fr[c, :, pl.ds(which * LANES, LANES)].astype(F32)

    depth = (chunks - 1) * pair
    bands = [pl.ds(i * (width // 4), width // 4) for i in range(4)]

    def input_grads(i):
        at_rows = pl.ds(i * tile, tile)
        for band in bands:
            dxa[at_rows, band] = lax.dot_general(
                db[at_rows, pl.ds(0, depth)], w[band, pl.ds(0, depth)], NT, preferred_element_type=F32)

    end = pl.ds(depth, pair)

    def input_pair(q):
        at_rows = pl.ds(q * tile, tile)
        for band in bands:
            value = lax.dot_general(db[at_rows, end], w[band, end], NT, preferred_element_type=F32)
            dxb[at_rows, band] = (dxa[at_rows, band] + value).astype(BF16)
        copies.start(("k", q), dxb.at[slot(2 * q + 1)], xk.at[q], core)

    left, right = pl.ds(0, width * 3 // 4), pl.ds(width * 3 // 4, width // 4)
    routes = {
        3: (("y", 0, left, across), ("x", 2, right, beside)),
        1: (("y", 1, left, across),),
        2: (("x", 3, right, beside),),
        0: (),
    }

    def core_sum(q):
        copies.arrived(("k", q), xk.at[q], core)
        xk[q] = add(xk[q], dxb[slot(2 * q), :])
        for name, place, part, device in routes[q]:
            copies.start(("q", place), xk.at[q, :, part], xq.at[place, :, part], device)

    def turn_corner(place, q, part, to, device):
        copies.arrived(("q", place), xq.at[place, :, part], device)
        xq[place, :, part] = add(xq[place, :, part], xk[q, :, part])
        copies.start(("q", to), xq.at[place, :, part], xq.at[to, :, part], device)

    def finish_input(places, part):
        total = xk[0, :, part].astype(F32)
        for place in places:
            copies.arrived(("q", place), xq.at[place, :, part], core)
            total = total + xq[place, :, part].astype(F32)
        gx[:, part] = total.astype(BF16)

    lap = 13.5 + (n - 4) * 6.4

    def passed(c, step, side):
        if c == 0 and step == 0 and side == 0:
            return 6.5
        return 8.3 + c * lap + (2 * step + side) * 3.2

    def begins(c):
        return passed(c, n - 2, 1) + 2.2 + 2 * c

    at(0.0, own_first, 0)
    at(0.1, swap_weights, 0)
    for to in ("core", "across", "beside"):
        at(0.2, own_block, "e", to)
    at(0.5, own_first, 1)
    at(5.0, own_second, 0)
    at(5.5, swap_weights, 1)
    at(5.6, swap_cotangent, 0)
    at(7.0, from_core, "e")
    at(7.1, turn, 0, 1)
    at(12.0, from_beside, "e", 0)
    at(13.5, from_across, "e")
    at(17.6, from_beside, "e", 1)
    for to in ("core", "across"):
        at(18.2, own_block, "l", to)
    at(19.0, turn, 2, 4)
    at(20.0, own_second, 1)
    for c in range(2, chunks):
        at(20.1 + (c - 2) * lap, swap_weights, c)
        at(20.2 + (c - 2) * lap, own_first, c)
        at(28.4 + (c - 2) * lap, own_second, c)
    for c in range(1, chunks):
        at(20.3, swap_cotangent, c)
    at(20.4, own_block, "l", "beside")
    for c in range(chunks):
        for step in range(n - 1):
            for side in range(2):
                at(passed(c, step, side), pass_weights, c, step, side)
    at(begins(0) - 1.0, from_diagonal, "e")
    at(begins(0) - 0.9, third_block, "e")
    at(begins(0) - 0.8, turn, 6, 3)
    at(begins(0) - 0.7, rest_blocks, "e")
    at(begins(0) - 0.6, turn, 5, 7)
    at(30.0, from_core, "l")
    at(38.0, from_across, "l")
    at(43.5, from_beside, "l", 0)
    at(43.6, from_beside, "l", 1)
    at(46.0, third_block, "l")
    at(51.0, from_diagonal, "l")
    at(52.5, rest_blocks, "l")
    corners = n - 1 - n // 2
    forwarded = passed(chunks - 1, max(n - 3, 0), 1)
    for c in range(chunks):
        start = begins(c)
        at(start - 0.2, collect, c)
        at(start - 0.1, got_cotangent, c)
        at(start, early, c)
        for i in range(n):
            at(start + (1.8 if c == 0 else 0.2) + 0.1 * i, weight_grads, c, i)
        first_sum = start + 7.0 + 2.5 * min(c, 1) + 1.5 * max(c - 1, 0)
        settled = max(first_sum + 11.5 + 4.0 * (chunks - 1 - c) + (n - 4) * 5.6, forwarded + 7.8)
        for rank, side in enumerate((1, 0)):
            for step in range(n - 2):
                at(first_sum + (2 * step + rank) * 2.8, pass_sums, c, step, side, True)
            for step in range(corners):
                moment = first_sum + 5.0 + (2 * step + rank) * 2.8
                at(max(moment, forwarded + 0.5 + 0.01 * rank + 0.02 * step), pass_sums, c, step, side, False)
            at(settled + rank * 2.8, settle, c, side)
        at(settled + 6.5, finish, c)
        if c < chunks - 1:
            at(max(50.2 + c, start + 1.0), late, c, 0)
            at(max(54.0 + c, start + 1.1), late, c, 1)
    tail = begins(chunks - 1)
    for i in range(tiles):
        at(begins(chunks - 2) + 4.6 + 0.9 * i, input_grads, i)
    at(tail + 5.0, late, chunks - 1, 1)
    at(tail + 5.1, late, chunks - 1, 0)
    for i, q in enumerate((3, 1, 2, 0)):
        at(tail + 0.25 + i * 0.1, input_pair, q)
        at(tail + 0.46 + i * 0.1, core_sum, q)
    at(tail + 8.0, turn_corner, 2, 1, right, 5, across)
    at(tail + 14.0, turn_corner, 0, 2, left, 4, beside)
    at(tail + 25.0, finish_input, (3, 5), right)
    at(tail + 26.0, finish_input, (1, 4), left)
    at(tail + 26.5, got_hidden)
    for _, _, action in sorted(plan, key=lambda entry: entry[:2]):
        action()
    copies.drain()
    local.drain()
    assert len(copies.index) <= ssem.shape[0] and len(local.copies) <= lsem.shape[0]


def store_kernel(tp_count, hm, hr, gxv, g, hid, gx, og, ou, sem):
    tp, x = lax.axis_index("tp"), lax.rem(lax.axis_index("fs"), 2)
    tokens, half = gxv.shape[0], hm.shape[1]
    local = Locals(sem)
    for side in range(2):
        lane = pl.ds(pl.multiple_of((x if side == 0 else 1 - x) * half, LANES), half)
        for which, out in enumerate((og, ou)):
            local.start(("o", which, side), g.at[which, side], out.at[:, lane])
        for m in range(tp_count):
            src = (hm, hr)[side].at[pl.ds(m * tokens, tokens)]
            local.start(("h", side, m), src, hid.at[aligned(flips(tp, m) * tokens, tokens), lane])
    local.start("gx", gxv, gx)
    local.drain()


def local_part(fs_count, tp_count, x_late, x_early, d_hidden, w_gate, w_up, gate_sum, up_sum):
    n = fs_count // 2
    tokens, width = x_early.shape
    rows, cols = w_gate.shape
    half = cols // 2
    chunks = half // LANES
    group = tp_count * tokens
    pair = 2 * LANES
    remote = chunks * (4 * (n - 1) + 4 * n + tp_count + 3) + 2 * 12 + tp_count + 6
    locals_count = 4 * chunks + 2 + tp_count + 4
    any_spec = pl.BlockSpec(memory_space=pl.ANY)
    vmem_spec = pl.BlockSpec(memory_space=pltpu.VMEM)
    results = pl.pallas_call(
        functools.partial(layer_kernel, fs_count, tp_count),
        out_shape=(
            jax.ShapeDtypeStruct((group, half), BF16),
            jax.ShapeDtypeStruct((group, half), BF16),
            jax.ShapeDtypeStruct(x_early.shape, BF16),
            jax.ShapeDtypeStruct((2, 2, rows, half), F32),
        ),
        in_specs=[any_spec] * 7,
        out_specs=(vmem_spec,) * 4,
        scratch_shapes=[
            pltpu.VMEM((width, 2 * half), BF16),
            pltpu.VMEM((rows, 2 * half), BF16),
            pltpu.VMEM((2 * group, width), BF16),
            pltpu.VMEM((2 * group, width), BF16),
            pltpu.VMEM((width, 2 * group), BF16),
            pltpu.VMEM((2 * group, half), BF16),
            pltpu.VMEM((2 * group, 2 * half), BF16),
            pltpu.VMEM((width, 2 * half), BF16),
            pltpu.VMEM((2, width, 2 * half), BF16),
            pltpu.VMEM((2 * group, width), F32),
            pltpu.VMEM((2 * group, width), BF16),
            pltpu.VMEM((tp_count, tokens, width), BF16),
            pltpu.VMEM((6, tokens, width), BF16),
            pltpu.VMEM((group, half), BF16),
            pltpu.VMEM((chunks, rows, pair), BF16),
            pltpu.VMEM((chunks, rows, pair), BF16),
            pltpu.SemaphoreType.DMA((remote,)),
            pltpu.SemaphoreType.DMA((remote,)),
            pltpu.SemaphoreType.DMA((locals_count,)),
        ],
        compiler_params=pltpu.CompilerParams(
            collective_id=0, has_side_effects=True, vmem_limit_bytes=58 * 1024 * 1024),
        name="layer",
    )(x_late, x_early, d_hidden, w_gate, w_up, gate_sum, up_sum)
    return pl.pallas_call(
        functools.partial(store_kernel, tp_count),
        out_shape=(
            jax.ShapeDtypeStruct((group, cols), BF16),
            jax.ShapeDtypeStruct(x_early.shape, BF16),
            jax.ShapeDtypeStruct(gate_sum.shape, F32),
            jax.ShapeDtypeStruct(up_sum.shape, F32),
        ),
        in_specs=[vmem_spec] * 4,
        out_specs=(any_spec,) * 4,
        scratch_shapes=[pltpu.SemaphoreType.DMA((2 * tp_count + 5,))],
        name="store",
    )(*results)


def solution(mesh):
    return jax.shard_map(
        functools.partial(local_part, mesh.shape["fs"], mesh.shape["tp"]),
        mesh=mesh,
        in_specs=(
            P(("fs", "tp"), None),
            P(("fs", "tp"), None),
            P("fs", "tp"),
            P("fs", "tp"),
            P("fs", "tp"),
            P("fs", "tp"),
            P("fs", "tp"),
        ),
        out_specs=(P("fs", "tp"), P(("fs", "tp"), None), P("fs", "tp"), P("fs", "tp")),
        check_vma=False,
    )
```

```python
import functools

import jax
import jax.numpy as jnp
from jax import lax
from jax.experimental import pallas as pl
from jax.experimental.pallas import tpu as pltpu
from jax.sharding import PartitionSpec as P

MESH = pl.DeviceIdType.MESH
F32 = jnp.float32
BF16 = jnp.bfloat16
LANES = 128
POOL = 48


def under(when, action):
    if when is None:
        action()
    else:
        pl.when(when)(action)


class Copies:
    def __init__(self, send_sem, recv_sem):
        self.send_sem, self.recv_sem = send_sem, recv_sem
        self.index, self.total, self.started, self.flying = {}, 0, 0, {}

    def number(self, key, count=1):
        if key not in self.index:
            self.index[key] = self.total
            self.total += count
        return self.index[key]

    def make(self, key, src, dst, device, send_at=0):
        at = self.number(key) if isinstance(key, tuple) else key
        return pltpu.make_async_remote_copy(
            src_ref=src, dst_ref=dst, send_sem=self.send_sem.at[send_at], recv_sem=self.recv_sem.at[at],
            device_id=device, device_id_type=MESH,
        )

    def start(self, key, src, dst, device, when=None):
        send_at = self.started % POOL
        self.settle(send_at)
        copy = self.make(key, src, dst, device, send_at)
        self.flying[send_at] = copy, when
        self.started += 1
        under(when, copy.start)

    def arrived(self, key, dst, device):
        self.make(key, dst, dst, device).wait_recv()

    def settle(self, send_at):
        if send_at in self.flying:
            copy, when = self.flying.pop(send_at)
            under(when, copy.wait_send)

    def drain(self):
        for send_at in sorted(self.flying):
            self.settle(send_at)


class Locals:
    def __init__(self, sem):
        self.sem, self.copies = sem, {}

    def start(self, key, src, dst):
        copy = pltpu.make_async_copy(src, dst, self.sem.at[len(self.copies)])
        self.copies[key] = [copy, False]
        copy.start()

    def wait(self, key):
        entry = self.copies[key]
        if not entry[1]:
            entry[1] = True
            entry[0].wait()

    def drain(self):
        for key in self.copies:
            self.wait(key)


def flip(index, bit):
    return jnp.where(lax.rem(lax.div(index, bit), 2) == 0, index + bit, index - bit)


def flips(index, mask):
    for bit in (1, 2):
        if mask & bit:
            index = flip(index, bit)
    return index


def aligned(value, size):
    return pl.ds(pl.multiple_of(value, size), size)


NT = (((1,), (1,)), ((), ()))


def layer_kernel(
    fs_count, tp_count, xl, xe, dh, wg, wu, gs, us, hm, hr, gx, g,
    w, ws, te, tl, tt, ct, db, dw, rs, dxa, dxb, xk, xq, hs, fb, fr, ssem, rsem, lsem,
):
    fs, tp = lax.axis_index("fs"), lax.axis_index("tp")
    z, x = lax.div(fs, 2), lax.rem(fs, 2)
    n = fs_count // 2
    rows, cols = wg.shape
    tokens, width = xe.shape
    half = cols // 2
    chunks = half // LANES
    pair = 2 * LANES
    up = (jnp.minimum(z + 1, n - 1) * 2 + x, tp)
    down = (jnp.maximum(z - 1, 0) * 2 + x, tp)
    beside = (z * 2 + 1 - x, tp)
    across = (fs, flip(tp, 2))
    core = (fs, flip(tp, 1))
    far = {"core": core, "across": across, "beside": beside}
    copies, local = Copies(ssem, rsem), Locals(lsem)

    def cc(c):
        return pl.ds(c * pair, pair)

    def wrows(at, side):
        return aligned((at * 2 + side) * rows, rows)

    def slot(r):
        return pl.ds(r * tokens, tokens)

    for c in range(chunks):
        for name, src, at in (("g", wg, 0), ("u", wu, LANES)):
            lane = pl.ds(c * pair + at, LANES)
            local.start(("w", c, name), src.at[:, aligned(x * half + c * LANES, LANES)], w.at[wrows(z, x), lane])
            local.start(("ws", c, name), src.at[:, aligned((1 - x) * half + c * LANES, LANES)], ws.at[:, lane])
        if c == 0:
            local.start("te", xe, te.at[slot(0)])
    local.start("tl", xl, tl.at[slot(0)])
    for m in range(tp_count):
        src = dh.at[aligned(flips(tp, m) * tokens, tokens), pl.ds(pl.multiple_of(x * half, LANES), half)]
        local.start(("ct", m), src, ct.at[slot(m)])
    for side in range(2):
        lane = pl.ds(pl.multiple_of((x if side == 0 else 1 - x) * half, LANES), half)
        for which, src in enumerate((gs, us)):
            local.start(("g", which, side), src.at[:, lane], g.at[which, side])

    barrier = pltpu.get_barrier_semaphore()

    def greet(device):
        pl.semaphore_signal(barrier, inc=1, device_id=device, device_id_type=MESH)

    pl.when(z < n - 1)(lambda: greet(up))
    pl.when(z > 0)(lambda: greet(down))
    for device in far.values():
        greet(device)
    ends = jnp.where(z < n - 1, 1, 0) + jnp.where(z > 0, 1, 0)
    pl.semaphore_wait(barrier, len(far) + ends)

    plan = []

    def at(time, action, *args):
        plan.append((time, len(plan), functools.partial(action, *args)))

    ways = (("u", up, z < n - 1), ("d", down, z > 0))

    def own_first(c):
        local.wait(("w", c, "g"))
        local.wait(("w", c, "u"))
        ref = w.at[wrows(z, x), cc(c)]
        for name, device, when in ways:
            copies.start(copies.number(("w", c, 0), n) + z, ref, ref, device, when)

    def swap_weights(c):
        local.wait(("ws", c, "g"))
        local.wait(("ws", c, "u"))
        copies.start(("b", c), ws.at[:, cc(c)], w.at[wrows(z, x), cc(c)], beside)

    inner = (z > 0) & (z < n - 1)

    def own_second(c, where=None):
        def action():
            copies.arrived(("b", c), ref, beside)

        ref = w.at[wrows(z, 1 - x), cc(c)]
        under(where, action)
        for name, device, when in ways:
            copies.start(copies.number(("w", c, 1), n) + z, ref, ref, device, when if where is None else when & where)

    def weight_piece(c, step, side, name):
        origin = z - 1 - step if name == "u" else z + 1 + step
        has = origin >= 0 if name == "u" else origin <= n - 1
        origin = jnp.clip(origin, 0, n - 1)
        return w.at[wrows(origin, x if side == 0 else 1 - x), cc(c)], has, copies.number(("w", c, side), n) + origin

    def pass_weights(c, step, side):
        if step == n - 2:
            return
        for name, device, when in ways:
            ref, has, key = weight_piece(c, step, side, name)
            pl.when(has & when)(lambda: copies.arrived(key, ref, device))
            copies.start(key, ref, ref, device, has & when)

    def collect(c):
        for step in range(n - 1):
            for side in range(2):
                for name, device, when in ways:
                    ref, has, key = weight_piece(c, step, side, name)
                    if step < n - 2:
                        has = has & jnp.logical_not(when)
                    pl.when(has)(lambda: copies.arrived(key, ref, device))

    arrays = {"e": (te, xe, "te"), "l": (tl, xl, "tl")}

    def block(kind, r, part):
        first, size = (0, tokens) if part is None else part
        return arrays[kind][0].at[pl.ds(r * tokens + first, size)]

    def send_block(kind, to, src, dst, part=None):
        copies.start((kind, to, dst, part), block(kind, src, part), block(kind, dst, part), far[to])

    def got_block(kind, to, dst, part=None):
        copies.arrived((kind, to, dst, part), block(kind, dst, part), far[to])

    middle = tokens // 2
    halves = ((0, middle), (middle, middle))
    side_way = {"e": tokens // 8, "l": 0}
    last_part = {kind: (tokens - size, size) for kind, size in side_way.items()}
    corner = {kind: (halves[0], (middle, middle - size)) for kind, size in side_way.items()}

    def own_block(kind, to):
        local.wait(arrays[kind][2])
        dst = {"core": 1, "across": 2, "beside": 4}[to]
        for part in halves if to == "beside" else (None,):
            send_block(kind, to, 0, dst, part)

    def from_core(kind):
        got_block(kind, "core", 1)

    def from_across(kind):
        got_block(kind, "across", 2)
        if side_way[kind]:
            send_block(kind, "beside", 2, 6, last_part[kind])
        send_block(kind, "core", 2, 3)

    def from_beside(kind, half_at):
        got_block(kind, "beside", 4, halves[half_at])
        send_block(kind, "across", 4, 6, corner[kind][half_at])
        send_block(kind, "core", 4, 5, halves[half_at])

    def from_diagonal(kind):
        for part in corner[kind]:
            got_block(kind, "across", 6, part)
            send_block(kind, "core", 6, 7, part)
        if side_way[kind]:
            got_block(kind, "beside", 6, last_part[kind])
            send_block(kind, "core", 6, 7, last_part[kind])

    def third_block(kind):
        got_block(kind, "core", 3)

    def fifth_block(kind):
        for part in halves:
            got_block(kind, "core", 5, part)

    def rest_blocks(kind):
        for part in corner[kind] + ((last_part[kind],) if side_way[kind] else ()):
            got_block(kind, "core", 7, part)

    def turn(*blocks):
        for r in blocks:
            tt[:, slot(r)] = te[slot(r), :].T

    def swap_cotangent(c):
        lane = aligned((1 - x) * half + c * LANES, LANES)
        for m in range(tp_count):
            src = dh.at[aligned(flips(tp, m) * tokens, tokens), lane]
            dst = ct.at[slot(tp_count + m), pl.ds(c * LANES, LANES)]
            copies.start(("c", c, m), src, dst, beside)

    def got_cotangent(c):
        for m in range(tp_count):
            local.wait(("ct", m))
            copies.arrived(("c", c, m), ct.at[slot(tp_count + m), pl.ds(c * LANES, LANES)], beside)

    tile = 2 * tokens
    tiles = 2 * tp_count * tokens // tile

    def early(c):
        def body(i, carry):
            at_rows = aligned(i * tile, tile)
            pre = jnp.dot(te[at_rows, :], w[:, cc(c)], preferred_element_type=F32)
            gate, up_part = pre[:, :LANES], pre[:, LANES:]
            s = jax.nn.sigmoid(gate)
            cot = ct[at_rows, pl.ds(c * LANES, LANES)].astype(F32)
            db[at_rows, pl.ds(c * pair, LANES)] = (cot * up_part * s * (1.0 + gate * (1.0 - s))).astype(BF16)
            db[at_rows, pl.ds(c * pair + LANES, LANES)] = (cot * gate * s).astype(BF16)
            return carry

        lax.fori_loop(0, tiles, body, 0, unroll=2)

    def late(c, first, i):
        out = hs if first else hm
        lane = pl.ds(c * LANES, LANES)
        at_rows = pl.ds(i * tile, tile)
        from_rows = pl.ds((first * tiles // 2 + i) * tile, tile)
        pre = jnp.dot(tl[from_rows, :], w[:, cc(c)], preferred_element_type=F32)
        gate, up_part = pre[:, :LANES], pre[:, LANES:]
        out[at_rows, lane] = (gate * jax.nn.sigmoid(gate) * up_part).astype(BF16)
        if first:
            copies.start(("h", c, i), hs.at[at_rows, lane], hr.at[at_rows, lane], beside)

    def got_hidden():
        for c in range(chunks):
            for i in range(tiles // 2):
                at_rows = pl.ds(i * tile, tile)
                copies.arrived(("h", c, i), hr.at[at_rows, pl.ds(c * LANES, LANES)], beside)

    def sum_key(c, side, d, target, receiver):
        base = copies.number(("r", c, side), n + 1)
        return base + jnp.where((d == 1) & (target == receiver), n, target)

    def beyond(d, target):
        return jnp.where(d == 0, target - z, z - target) > 0

    def onward(d):
        to = jnp.clip(jnp.where(d == 0, z + 1, z - 1), 0, n - 1)
        return to, (to * 2 + x, tp)

    def srows(target, side):
        return wrows(target, x if side == 0 else 1 - x)

    def trows(target):
        return aligned(target * 2 * rows, 2 * rows)

    def grad_target(i):
        return jnp.where(z < n // 2, n - 1 - i, i)

    def weight_grads(c, i, side, send=True):
        piece = srows(grad_target(i), side)
        dw[piece, cc(c)] = jnp.dot(tt[piece, :], db[:, cc(c)], preferred_element_type=F32).astype(BF16)
        if send:
            send_grads(c, i, side)

    def send_grads(c, i, side):
        target = grad_target(i)
        piece = srows(target, side)
        d = jnp.where(z == 0, 0, 1)
        to, device = onward(d)
        when = jnp.logical_not(inner) & beyond(d, target)
        copies.start(sum_key(c, side, d, target, to), dw.at[piece, cc(c)], rs.at[d, piece, cc(c)], device, when)

    def add(a, b):
        return (a.astype(F32) + b.astype(F32)).astype(BF16)

    def pass_sums(c, step, side, near):
        d = jnp.where(z < n // 2, 0, 1) if near else jnp.where(z < n // 2, 1, 0)
        target = jnp.where(d == 0, n - 1 - step, step)
        passes = inner & beyond(d, target)
        to, device = onward(d)
        ref = rs.at[d, srows(target, side), cc(c)]
        own = dw.at[srows(target, side), cc(c)]

        def action():
            copies.arrived(sum_key(c, side, d, target, z), ref, device)
            ref[...] = add(ref[...], own[...])

        pl.when(passes)(action)
        copies.start(sum_key(c, side, d, target, to), ref, ref, device, passes)

    def settle(c, side):
        rows_here = srows(z, side)
        for d, behind in ((0, z > 0), (1, z < n - 1)):
            ref = rs.at[d, rows_here, cc(c)]

            def take():
                copies.arrived(sum_key(c, side, d, z, z), ref, beside)

            def blank():
                ref[...] = jnp.zeros((rows, pair), BF16)

            pl.when(behind)(take)
            pl.when(jnp.logical_not(behind))(blank)
        total = dw[rows_here, cc(c)].astype(F32)
        for d in range(2):
            total = total + rs[d, rows_here, cc(c)].astype(F32)
        if side == 1:
            fb[c] = total.astype(BF16)
            copies.start(("f", c), fb.at[c], fr.at[c], beside)
            return
        lane = pl.ds(c * LANES, LANES)
        for which in range(2):
            local.wait(("g", which, 0))
            g[which, 0, :, lane] = g[which, 0, :, lane] + total[:, which * LANES : (which + 1) * LANES]

    def finish(c):
        copies.arrived(("f", c), fr.at[c], beside)
        lane = pl.ds(c * LANES, LANES)
        for which in range(2):
            local.wait(("g", which, 1))
            g[which, 1, :, lane] = g[which, 1, :, lane] + fr[c, :, pl.ds(which * LANES, LANES)].astype(F32)

    depth = (chunks - 1) * pair
    bands = [pl.ds(i * (width // 4), width // 4) for i in range(4)]

    def input_grads(i):
        at_rows = pl.ds(i * tile, tile)
        for band in bands:
            dxa[at_rows, band] = lax.dot_general(
                db[at_rows, pl.ds(0, depth)], w[band, pl.ds(0, depth)], NT, preferred_element_type=F32)

    end = pl.ds(depth, pair)

    def input_pair(q):
        at_rows = pl.ds(q * tile, tile)
        for band in bands:
            value = lax.dot_general(db[at_rows, end], w[band, end], NT, preferred_element_type=F32)
            dxb[at_rows, band] = (dxa[at_rows, band] + value).astype(BF16)
        copies.start(("k", q), dxb.at[slot(2 * q + 1)], xk.at[q], core)

    unit = width // 16
    parts = (pl.ds(0, 7 * unit), pl.ds(7 * unit, 7 * unit), pl.ds(14 * unit, 2 * unit))
    routes = {
        3: (("y", 0, 0), ("y", 0, 1), ("x", 2, 2)),
        1: (("y", 1, 0), ("y", 1, 1)),
        2: (("x", 3, 2),),
        0: (),
    }

    def core_sum(q):
        copies.arrived(("k", q), xk.at[q], core)
        xk[q] = add(xk[q], dxb[slot(2 * q), :])
        for name, place, at_part in routes[q]:
            part = parts[at_part]
            device = across if name == "y" else beside
            copies.start(("q", place, at_part), xk.at[q, :, part], xq.at[place, :, part], device)

    def turn_corner(at_part):
        place, q, to, device = (2, 1, 5, across) if at_part == 2 else (0, 2, 4, beside)
        part = parts[at_part]
        copies.arrived(("q", place, at_part), xq.at[place, :, part], device)
        xq[place, :, part] = add(xq[place, :, part], xk[q, :, part])
        copies.start(("q", to, at_part), xq.at[place, :, part], xq.at[to, :, part], device)

    def finish_input(at_part):
        part = parts[at_part]
        total = xk[0, :, part].astype(F32)
        for place in (3, 5) if at_part == 2 else (1, 4):
            copies.arrived(("q", place, at_part), xq.at[place, :, part], core)
            total = total + xq[place, :, part].astype(F32)
        gx[:, part] = total.astype(BF16)

    lap = 13.5 + (n - 4) * 6.4

    def passed(c, step, side):
        if c == 0 and step == 0 and side == 0:
            return 6.5
        if c == 1 and step == 0 and side == 1:
            return begins(0) + 0.05
        if c == 1 and step == 1 and side == 0:
            return begins(0) + 0.2
        if c == chunks - 1 and step == 0:
            return passed(c - 1, n - 3, 1) + 0.2 + 0.1 * side
        if c == chunks - 1 and step == n - 3 and side == 1:
            return begins(c - 1) + 0.1
        return 8.3 + c * lap + (2 * step + side) * 3.2

    def begins(c):
        return 10.5 + c * (lap + 2) + (2 * n - 3) * 3.2

    at(0.0, own_first, 0)
    at(0.1, swap_weights, 0)
    for to in ("core", "across", "beside"):
        at(0.2, own_block, "e", to)
    at(0.5, own_first, 1)
    at(5.0, own_second, 0)
    at(5.5, swap_weights, 1)
    at(5.6, swap_cotangent, 0)
    at(7.0, from_core, "e")
    at(7.1, turn, 0, 1)
    at(12.0, from_beside, "e", 0)
    at(13.5, from_across, "e")
    at(17.6, from_beside, "e", 1)
    for to in ("core", "across"):
        at(18.2, own_block, "l", to)
    at(19.0, turn, 2, 4)
    at(20.0, own_second, 1)
    for c in range(2, chunks):
        at(20.1 + (c - 2) * lap, swap_weights, c)
        at(21.9 + (c - 2) * lap, own_first, c)
        at(begins(c - 2) + 0.08, own_second, c, jnp.logical_not(inner))
        at(passed(c - 1, max(n - 3, 0), 1) + 0.1, own_second, c, inner)
    at(20.25, own_block, "l", "beside")
    for c in range(1, chunks):
        at(20.3, swap_cotangent, c)
    for c in range(chunks):
        for step in range(n - 1):
            for side in range(2):
                at(passed(c, step, side), pass_weights, c, step, side)
    at(begins(0) - 1.0, from_diagonal, "e")
    at(begins(0) - 1.2, third_block, "e")
    at(begins(0) - 1.1, turn, 3)
    at(begins(0) - 0.8, fifth_block, "e")
    at(begins(0) - 0.75, turn, 6, 5)
    at(begins(0) - 0.7, rest_blocks, "e")
    at(begins(0) - 0.6, turn, 7)
    at(30.0, from_core, "l")
    at(35.0, from_beside, "l", 0)
    at(37.0, from_across, "l")
    at(40.0, from_beside, "l", 1)
    at(begins(chunks - 2) + 2.9, third_block, "l")
    at(begins(chunks - 2) + 2.9, fifth_block, "l")
    at(begins(chunks - 2) + 3.0, from_diagonal, "l")
    at(begins(chunks - 2) + 4.0, rest_blocks, "l")
    corners = n - 1 - n // 2
    forwarded = passed(chunks - 1, max(n - 3, 0), 1)
    tail = begins(chunks - 1)
    more = (n - 4) * 5.6
    for c in range(chunks):
        final, middle_one = c == chunks - 1, c == chunks - 2
        start = begins(c)
        at(start - 0.2, collect, c)
        at(start - 0.1, got_cotangent, c)
        at(start, early, c)
        for i in range(n):
            for side in (1, 0):
                held = middle_one and i == n - 2 and side == 0
                moment = start + (1.8 if c == 0 else 0.2) + 0.1 * i
                if final:
                    order = 2 * i - side + (2 if side == 0 and i == n - 3 else 0)
                    moment = tail + (0.08 - 0.01 * side if i == 0 else 0.6 + 0.001 * order if i < n - 1 else 0.66)
                at(moment, weight_grads, c, i, side, not held)
                if held:
                    at(tail + 0.10, send_grads, c, i, side)
        first_sum = start + (7.0 if c == 0 else 10.5)
        for rank, side in enumerate((1, 0)):
            for step in range(n - 2):
                moment = first_sum + (2 * step + rank) * 2.7
                if c == 0 and step == n - 3 and rank == 1:
                    moment = max(moment, begins(1) + 0.15)
                if middle_one and step == n - 3:
                    moment = tail + 0.12 + 0.44 * rank
                if final:
                    moment = tail + (0.65, 0.67, 0.73, 0.81)[min(2 * max(step - n + 4, 0) + rank, 3)] + 0.0001 * step
                at(moment, pass_sums, c, step, side, True)
            for step in range(corners):
                moment = first_sum + 4.0 + (2 * step + rank) * 2.8
                if final:
                    moment = tail + (0.71, 0.75)[rank] + 0.0001 * step
                elif middle_one:
                    moment = tail + 0.36 + 0.19 * rank + 0.0001 * step
                else:
                    moment = max(moment, forwarded + 0.5 + 0.01 * rank + 0.02 * step)
                at(moment, pass_sums, c, step, side, False)
        if final:
            at(tail + 0.80, settle, c, 1)
            at(tail + 0.85, settle, c, 0)
            at(tail + 0.89, finish, c)
        elif middle_one:
            at(tail + 0.63, settle, c, 1)
            at(tail + 0.74, settle, c, 0)
            at(tail + 0.87, finish, c)
        else:
            at(tail + 0.25, settle, c, 1)
            at(tail + 0.58, settle, c, 0)
            at(tail + 0.68, finish, c)
        if not final:
            for i in range(tiles // 2):
                at(begins(chunks - 2) + (3.5 if i < tiles // 4 else 4.2) + 0.01 * c, late, c, 1, i)
                at(tail + 0.76, late, c, 0, i)
    for i in range(tiles):
        at(begins(chunks - 2) + 4.6 + 0.1 * i, input_grads, i)
    for i in range(tiles // 2):
        at(tail + 0.52, late, chunks - 1, 1, i)
        at(tail + (0.69 if i == 0 else 0.72), late, chunks - 1, 0, i)
    for q, made, summed in ((3, 0.05, 0.2), (1, 0.06, 0.33), (2, 0.31, 0.5), (0, 0.34, 0.57)):
        at(tail + made, input_pair, q)
        at(tail + summed, core_sum, q)
    at(tail + 0.59, turn_corner, 2)
    at(tail + 0.64, turn_corner, 0)
    at(tail + 0.70, turn_corner, 1)
    at(tail + 0.82, finish_input, 2)
    at(tail + 0.83, finish_input, 0)
    at(tail + 0.86, finish_input, 1)
    at(tail + 0.88, got_hidden)
    for _, _, action in sorted(plan, key=lambda entry: entry[:2]):
        action()
    copies.drain()
    local.drain()
    assert copies.total <= rsem.shape[0] and len(local.copies) <= lsem.shape[0]


def store_kernel(tp_count, hm, hr, gxv, g, hid, gx, og, ou, sem):
    tp, x = lax.axis_index("tp"), lax.rem(lax.axis_index("fs"), 2)
    tokens, half = gxv.shape[0], hm.shape[1]
    local = Locals(sem)
    for side in range(2):
        lane = pl.ds(pl.multiple_of((x if side == 0 else 1 - x) * half, LANES), half)
        for which, out in enumerate((og, ou)):
            local.start(("o", which, side), g.at[which, side], out.at[:, lane])
        for m in range(tp_count):
            src = (hm, hr)[side].at[pl.ds(m * tokens, tokens)]
            local.start(("h", side, m), src, hid.at[aligned(flips(tp, m) * tokens, tokens), lane])
    local.start("gx", gxv, gx)
    local.drain()


def local_part(fs_count, tp_count, x_late, x_early, d_hidden, w_gate, w_up, gate_sum, up_sum):
    n = fs_count // 2
    tokens, width = x_early.shape
    rows, cols = w_gate.shape
    half = cols // 2
    chunks = half // LANES
    group = tp_count * tokens
    pair = 2 * LANES
    remote = chunks * (4 * n + tp_count + 6) + 40
    locals_count = 4 * chunks + 2 + tp_count + 4
    any_spec = pl.BlockSpec(memory_space=pl.ANY)
    vmem_spec = pl.BlockSpec(memory_space=pltpu.VMEM)
    results = pl.pallas_call(
        functools.partial(layer_kernel, fs_count, tp_count),
        out_shape=(
            pltpu.VMEM((group, half), BF16),
            pltpu.VMEM((group, half), BF16),
            pltpu.VMEM(x_early.shape, BF16),
            pltpu.VMEM((2, 2, rows, half), F32),
        ),
        in_specs=[any_spec] * 7,
        out_specs=(vmem_spec,) * 4,
        scratch_shapes=[
            pltpu.VMEM((width, 2 * half), BF16),
            pltpu.VMEM((rows, 2 * half), BF16),
            pltpu.VMEM((2 * group, width), BF16),
            pltpu.VMEM((2 * group, width), BF16),
            pltpu.VMEM((width, 2 * group), BF16),
            pltpu.VMEM((2 * group, half), BF16),
            pltpu.VMEM((2 * group, 2 * half), BF16),
            pltpu.VMEM((width, 2 * half), BF16),
            pltpu.VMEM((2, width, 2 * half), BF16),
            pltpu.VMEM((2 * group, width), F32),
            pltpu.VMEM((2 * group, width), BF16),
            pltpu.VMEM((tp_count, tokens, width), BF16),
            pltpu.VMEM((6, tokens, width), BF16),
            pltpu.VMEM((group, half), BF16),
            pltpu.VMEM((chunks, rows, pair), BF16),
            pltpu.VMEM((chunks, rows, pair), BF16),
            pltpu.SemaphoreType.DMA((POOL,)),
            pltpu.SemaphoreType.DMA((remote,)),
            pltpu.SemaphoreType.DMA((locals_count,)),
        ],
        compiler_params=pltpu.CompilerParams(
            collective_id=0, has_side_effects=True, vmem_limit_bytes=58 * 1024 * 1024),
        name="layer",
    )(x_late, x_early, d_hidden, w_gate, w_up, gate_sum, up_sum)
    return pl.pallas_call(
        functools.partial(store_kernel, tp_count),
        out_shape=(
            jax.ShapeDtypeStruct((group, cols), BF16),
            jax.ShapeDtypeStruct(x_early.shape, BF16),
            jax.ShapeDtypeStruct(gate_sum.shape, F32),
            jax.ShapeDtypeStruct(up_sum.shape, F32),
        ),
        in_specs=[vmem_spec] * 4,
        out_specs=(any_spec,) * 4,
        scratch_shapes=[pltpu.SemaphoreType.DMA((2 * tp_count + 5,))],
        name="store",
    )(*(pltpu.with_memory_space_constraint(value, pltpu.VMEM) for value in results))


def solution(mesh):
    return jax.shard_map(
        functools.partial(local_part, mesh.shape["fs"], mesh.shape["tp"]),
        mesh=mesh,
        in_specs=(
            P(("fs", "tp"), None),
            P(("fs", "tp"), None),
            P("fs", "tp"),
            P("fs", "tp"),
            P("fs", "tp"),
            P("fs", "tp"),
            P("fs", "tp"),
        ),
        out_specs=(P("fs", "tp"), P(("fs", "tp"), None), P("fs", "tp"), P("fs", "tp")),
        check_vma=False,
    )
```

```python
import functools

import jax
import jax.numpy as jnp
from jax import lax
from jax.experimental import pallas as pl
from jax.experimental.pallas import tpu as pltpu
from jax.sharding import PartitionSpec as P

MESH = pl.DeviceIdType.MESH
F32 = jnp.float32
BF16 = jnp.bfloat16
LANES = 128
POOL = 48


def under(when, action):
    if when is None:
        action()
    else:
        pl.when(when)(action)


class Copies:
    def __init__(self, send_sem, recv_sem):
        self.send_sem, self.recv_sem = send_sem, recv_sem
        self.index, self.total, self.started, self.flying = {}, 0, 0, {}

    def number(self, key, count=1):
        if key not in self.index:
            self.index[key] = self.total
            self.total += count
        return self.index[key]

    def make(self, key, src, dst, device, send_at=0):
        at = self.number(key) if isinstance(key, tuple) else key
        return pltpu.make_async_remote_copy(
            src_ref=src, dst_ref=dst, send_sem=self.send_sem.at[send_at], recv_sem=self.recv_sem.at[at],
            device_id=device, device_id_type=MESH,
        )

    def start(self, key, src, dst, device, when=None):
        send_at = self.started % POOL
        self.settle(send_at)
        copy = self.make(key, src, dst, device, send_at)
        self.flying[send_at] = copy, when
        self.started += 1
        under(when, copy.start)

    def arrived(self, key, dst, device):
        self.make(key, dst, dst, device).wait_recv()

    def settle(self, send_at):
        if send_at in self.flying:
            copy, when = self.flying.pop(send_at)
            under(when, copy.wait_send)

    def drain(self):
        for send_at in sorted(self.flying):
            self.settle(send_at)


class Locals:
    def __init__(self, sem):
        self.sem, self.copies = sem, {}

    def start(self, key, src, dst):
        copy = pltpu.make_async_copy(src, dst, self.sem.at[len(self.copies)])
        self.copies[key] = [copy, False]
        copy.start()

    def wait(self, key):
        entry = self.copies[key]
        if not entry[1]:
            entry[1] = True
            entry[0].wait()

    def drain(self):
        for key in self.copies:
            self.wait(key)


def flip(index, bit):
    return jnp.where(lax.rem(lax.div(index, bit), 2) == 0, index + bit, index - bit)


def flips(index, mask):
    for bit in (1, 2):
        if mask & bit:
            index = flip(index, bit)
    return index


def aligned(value, size):
    return pl.ds(pl.multiple_of(value, size), size)


NT = (((1,), (1,)), ((), ()))


def layer_kernel(
    fs_count, tp_count, xl, xe, dh, wg, wu, gs, us, hm, hr, gx, g,
    w, ws, te, tl, tt, ct, db, dw, rs, dxa, dxb, xk, xq, hs, fb, fr, ssem, rsem, lsem,
):
    fs, tp = lax.axis_index("fs"), lax.axis_index("tp")
    z, x = lax.div(fs, 2), lax.rem(fs, 2)
    n = fs_count // 2
    rows, cols = wg.shape
    tokens, width = xe.shape
    half = cols // 2
    chunks = half // LANES
    pair = 2 * LANES
    up = (jnp.minimum(z + 1, n - 1) * 2 + x, tp)
    down = (jnp.maximum(z - 1, 0) * 2 + x, tp)
    beside = (z * 2 + 1 - x, tp)
    across = (fs, flip(tp, 2))
    core = (fs, flip(tp, 1))
    far = {"core": core, "across": across, "beside": beside}
    copies, local = Copies(ssem, rsem), Locals(lsem)

    def cc(c):
        return pl.ds(c * pair, pair)

    def wrows(at, side):
        return aligned((at * 2 + side) * rows, rows)

    def slot(r):
        return pl.ds(r * tokens, tokens)

    barrier = pltpu.get_barrier_semaphore()

    def greet(device):
        pl.semaphore_signal(barrier, inc=1, device_id=device, device_id_type=MESH)

    pl.when(z < n - 1)(lambda: greet(up))
    pl.when(z > 0)(lambda: greet(down))
    for device in far.values():
        greet(device)
    for c in range(chunks):
        for name, src, at in (("g", wg, 0), ("u", wu, LANES)):
            lane = pl.ds(c * pair + at, LANES)
            local.start(("w", c, name), src.at[:, aligned(x * half + c * LANES, LANES)], w.at[wrows(z, x), lane])
            local.start(("ws", c, name), src.at[:, aligned((1 - x) * half + c * LANES, LANES)], ws.at[:, lane])
        if c == 0:
            local.start("te", xe, te.at[slot(0)])
    local.start("tl", xl, tl.at[slot(0)])
    for m in range(tp_count):
        src = dh.at[aligned(flips(tp, m) * tokens, tokens), pl.ds(pl.multiple_of(x * half, LANES), half)]
        local.start(("ct", m), src, ct.at[slot(m)])
    for side in range(2):
        lane = pl.ds(pl.multiple_of((x if side == 0 else 1 - x) * half, LANES), half)
        for which, src in enumerate((gs, us)):
            local.start(("g", which, side), src.at[:, lane], g.at[which, side])

    ends = jnp.where(z < n - 1, 1, 0) + jnp.where(z > 0, 1, 0)
    pl.semaphore_wait(barrier, len(far) + ends)

    plan = []

    def at(time, action, *args):
        plan.append((time, len(plan), functools.partial(action, *args)))

    ways = (("u", up, z < n - 1), ("d", down, z > 0))

    def own_first(c):
        local.wait(("w", c, "g"))
        local.wait(("w", c, "u"))
        ref = w.at[wrows(z, x), cc(c)]
        for name, device, when in ways:
            copies.start(copies.number(("w", c, 0), n) + z, ref, ref, device, when)

    def swap_weights(c):
        local.wait(("ws", c, "g"))
        local.wait(("ws", c, "u"))
        copies.start(("b", c), ws.at[:, cc(c)], w.at[wrows(z, x), cc(c)], beside)

    inner = (z > 0) & (z < n - 1)

    def own_second(c, where=None):
        def action():
            copies.arrived(("b", c), ref, beside)

        ref = w.at[wrows(z, 1 - x), cc(c)]
        under(where, action)
        for name, device, when in ways:
            copies.start(copies.number(("w", c, 1), n) + z, ref, ref, device, when if where is None else when & where)

    def weight_piece(c, step, side, name):
        origin = z - 1 - step if name == "u" else z + 1 + step
        has = origin >= 0 if name == "u" else origin <= n - 1
        origin = jnp.clip(origin, 0, n - 1)
        return w.at[wrows(origin, x if side == 0 else 1 - x), cc(c)], has, copies.number(("w", c, side), n) + origin

    def pass_weights(c, step, side):
        if step == n - 2:
            return
        for name, device, when in ways:
            ref, has, key = weight_piece(c, step, side, name)
            pl.when(has & when)(lambda: copies.arrived(key, ref, device))
            copies.start(key, ref, ref, device, has & when)

    def collect(c):
        for step in range(n - 1):
            for side in range(2):
                for name, device, when in ways:
                    ref, has, key = weight_piece(c, step, side, name)
                    if step < n - 2:
                        has = has & jnp.logical_not(when)
                    pl.when(has)(lambda: copies.arrived(key, ref, device))

    arrays = {"e": (te, xe, "te"), "l": (tl, xl, "tl")}

    def block(kind, r, part):
        first, size = (0, tokens) if part is None else part
        return arrays[kind][0].at[pl.ds(r * tokens + first, size)]

    def send_block(kind, to, src, dst, part=None):
        copies.start((kind, to, dst, part), block(kind, src, part), block(kind, dst, part), far[to])

    def got_block(kind, to, dst, part=None):
        copies.arrived((kind, to, dst, part), block(kind, dst, part), far[to])

    middle = tokens // 2
    halves = ((0, middle), (middle, middle))
    side_way = {"e": tokens // 8, "l": 0}
    last_part = {kind: (tokens - size, size) for kind, size in side_way.items()}
    corner = {kind: (halves[0], (middle, middle - size)) for kind, size in side_way.items()}

    def own_block(kind, to):
        local.wait(arrays[kind][2])
        dst = {"core": 1, "across": 2, "beside": 4}[to]
        for part in halves if to == "beside" else (None,):
            send_block(kind, to, 0, dst, part)

    def from_core(kind):
        got_block(kind, "core", 1)

    def from_across(kind):
        got_block(kind, "across", 2)
        if side_way[kind]:
            send_block(kind, "beside", 2, 6, last_part[kind])
        send_block(kind, "core", 2, 3)

    def from_beside(kind, half_at):
        got_block(kind, "beside", 4, halves[half_at])
        send_block(kind, "across", 4, 6, corner[kind][half_at])
        send_block(kind, "core", 4, 5, halves[half_at])

    def from_diagonal(kind):
        for part in corner[kind]:
            got_block(kind, "across", 6, part)
            send_block(kind, "core", 6, 7, part)
        if side_way[kind]:
            got_block(kind, "beside", 6, last_part[kind])
            send_block(kind, "core", 6, 7, last_part[kind])

    def third_block(kind):
        got_block(kind, "core", 3)

    def fifth_block(kind):
        for part in halves:
            got_block(kind, "core", 5, part)

    def rest_blocks(kind):
        for part in corner[kind] + ((last_part[kind],) if side_way[kind] else ()):
            got_block(kind, "core", 7, part)

    def turn(*blocks):
        for r in blocks:
            tt[:, slot(r)] = te[slot(r), :].T

    def swap_cotangent(c):
        lane = aligned((1 - x) * half + c * LANES, LANES)
        for m in range(tp_count):
            src = dh.at[aligned(flips(tp, m) * tokens, tokens), lane]
            dst = ct.at[slot(tp_count + m), pl.ds(c * LANES, LANES)]
            copies.start(("c", c, m), src, dst, beside)

    def got_cotangent(c):
        for m in range(tp_count):
            local.wait(("ct", m))
            copies.arrived(("c", c, m), ct.at[slot(tp_count + m), pl.ds(c * LANES, LANES)], beside)

    tile = 2 * tokens
    tiles = 2 * tp_count * tokens // tile

    def early(c, low=0, high=tiles):
        def body(i, carry):
            at_rows = aligned(i * tile, tile)
            pre = jnp.dot(te[at_rows, :], w[:, cc(c)], preferred_element_type=F32)
            gate, up_part = pre[:, :LANES], pre[:, LANES:]
            s = jax.nn.sigmoid(gate)
            cot = ct[at_rows, pl.ds(c * LANES, LANES)].astype(F32)
            db[at_rows, pl.ds(c * pair, LANES)] = (cot * up_part * s * (1.0 + gate * (1.0 - s))).astype(BF16)
            db[at_rows, pl.ds(c * pair + LANES, LANES)] = (cot * gate * s).astype(BF16)
            return carry

        lax.fori_loop(low, high, body, 0, unroll=2 if (high - low) % 2 == 0 else 1)

    def late(c, first, i):
        out = hs if first else hm
        lane = pl.ds(c * LANES, LANES)

        def body(at_tile, carry):
            at_rows = aligned(at_tile * tile, tile)
            from_rows = aligned((first * tiles // 2 + at_tile) * tile, tile)
            pre = jnp.dot(tl[from_rows, :], w[:, cc(c)], preferred_element_type=F32)
            gate, up_part = pre[:, :LANES], pre[:, LANES:]
            out[at_rows, lane] = (gate * jax.nn.sigmoid(gate) * up_part).astype(BF16)
            return carry

        lax.fori_loop(i, i + 1, body, 0)
        if first:
            at_rows = pl.ds(i * tile, tile)
            copies.start(("h", c, i), hs.at[at_rows, lane], hr.at[at_rows, lane], beside)

    def got_hidden():
        for c in range(chunks):
            for i in range(tiles // 2):
                at_rows = pl.ds(i * tile, tile)
                copies.arrived(("h", c, i), hr.at[at_rows, pl.ds(c * LANES, LANES)], beside)

    def sum_key(c, side, d, target, receiver):
        base = copies.number(("r", c, side), n + 1)
        return base + jnp.where((d == 1) & (target == receiver), n, target)

    def beyond(d, target):
        return jnp.where(d == 0, target - z, z - target) > 0

    def onward(d):
        to = jnp.clip(jnp.where(d == 0, z + 1, z - 1), 0, n - 1)
        return to, (to * 2 + x, tp)

    def srows(target, side):
        return wrows(target, x if side == 0 else 1 - x)

    def trows(target):
        return aligned(target * 2 * rows, 2 * rows)

    def grad_target(i):
        return jnp.where(z < n // 2, n - 1 - i, i)

    def weight_grads(c, i, side, send=True):
        piece = srows(grad_target(i), side)
        dw[piece, cc(c)] = jnp.dot(tt[piece, :], db[:, cc(c)], preferred_element_type=F32).astype(BF16)
        if send:
            send_grads(c, i, side)

    def send_grads(c, i, side):
        target = grad_target(i)
        piece = srows(target, side)
        d = jnp.where(z == 0, 0, 1)
        to, device = onward(d)
        when = jnp.logical_not(inner) & beyond(d, target)
        copies.start(sum_key(c, side, d, target, to), dw.at[piece, cc(c)], rs.at[d, piece, cc(c)], device, when)

    def add(a, b):
        return (a.astype(F32) + b.astype(F32)).astype(BF16)

    def pass_sums(c, step, side, near):
        d = jnp.where(z < n // 2, 0, 1) if near else jnp.where(z < n // 2, 1, 0)
        target = jnp.where(d == 0, n - 1 - step, step)
        passes = inner & beyond(d, target)
        to, device = onward(d)
        ref = rs.at[d, srows(target, side), cc(c)]
        own = dw.at[srows(target, side), cc(c)]

        def action():
            copies.arrived(sum_key(c, side, d, target, z), ref, device)
            ref[...] = add(ref[...], own[...])

        pl.when(passes)(action)
        copies.start(sum_key(c, side, d, target, to), ref, ref, device, passes)

    def settle(c, side):
        rows_here = srows(z, side)
        for d, behind in ((0, z > 0), (1, z < n - 1)):
            ref = rs.at[d, rows_here, cc(c)]

            def take():
                copies.arrived(sum_key(c, side, d, z, z), ref, beside)

            def blank():
                ref[...] = jnp.zeros((rows, pair), BF16)

            pl.when(behind)(take)
            pl.when(jnp.logical_not(behind))(blank)
        total = dw[rows_here, cc(c)].astype(F32)
        for d in range(2):
            total = total + rs[d, rows_here, cc(c)].astype(F32)
        if side == 1:
            fb[c] = total.astype(BF16)
            copies.start(("f", c), fb.at[c], fr.at[c], beside)
            return
        lane = pl.ds(c * LANES, LANES)
        for which in range(2):
            local.wait(("g", which, 0))
            g[which, 0, :, lane] = g[which, 0, :, lane] + total[:, which * LANES : (which + 1) * LANES]

    def finish(c):
        copies.arrived(("f", c), fr.at[c], beside)
        lane = pl.ds(c * LANES, LANES)
        for which in range(2):
            local.wait(("g", which, 1))
            g[which, 1, :, lane] = g[which, 1, :, lane] + fr[c, :, pl.ds(which * LANES, LANES)].astype(F32)

    depth = (chunks - 1) * pair
    bands = [pl.ds(i * (width // 4), width // 4) for i in range(4)]

    def input_grads(i):
        at_rows = pl.ds(i * tile, tile)
        for band in bands:
            dxa[at_rows, band] = lax.dot_general(
                db[at_rows, pl.ds(0, depth)], w[band, pl.ds(0, depth)], NT, preferred_element_type=F32)

    end = pl.ds(depth, pair)

    def input_pair(q):
        at_rows = pl.ds(q * tile, tile)
        for band in bands:
            value = lax.dot_general(db[at_rows, end], w[band, end], NT, preferred_element_type=F32)
            dxb[at_rows, band] = (dxa[at_rows, band] + value).astype(BF16)
        copies.start(("k", q), dxb.at[slot(2 * q + 1)], xk.at[q], core)

    unit = width // 16
    parts = (pl.ds(0, 7 * unit), pl.ds(7 * unit, 7 * unit), pl.ds(14 * unit, 2 * unit))
    routes = {
        3: (("y", 0, 0), ("y", 0, 1), ("x", 2, 2)),
        1: (("y", 1, 0), ("y", 1, 1)),
        2: (("x", 3, 2),),
        0: (),
    }

    def core_sum(q):
        copies.arrived(("k", q), xk.at[q], core)
        xk[q] = add(xk[q], dxb[slot(2 * q), :])
        for name, place, at_part in routes[q]:
            part = parts[at_part]
            device = across if name == "y" else beside
            copies.start(("q", place, at_part), xk.at[q, :, part], xq.at[place, :, part], device)

    def turn_corner(at_part):
        place, q, to, device = (2, 1, 5, across) if at_part == 2 else (0, 2, 4, beside)
        part = parts[at_part]
        copies.arrived(("q", place, at_part), xq.at[place, :, part], device)
        xq[place, :, part] = add(xq[place, :, part], xk[q, :, part])
        copies.start(("q", to, at_part), xq.at[place, :, part], xq.at[to, :, part], device)

    def finish_input(at_part):
        part = parts[at_part]
        total = xk[0, :, part].astype(F32)
        for place in (3, 5) if at_part == 2 else (1, 4):
            copies.arrived(("q", place, at_part), xq.at[place, :, part], core)
            total = total + xq[place, :, part].astype(F32)
        gx[:, part] = total.astype(BF16)

    lap = 13.5 + (n - 4) * 6.4

    def passed(c, step, side):
        if c == 0 and step == 0 and side == 0:
            return 6.5
        if c == 1 and step == 0 and side == 1:
            return begins(0) + 0.05
        if c == 1 and step == 1 and side == 0:
            return begins(0) + 0.2
        if c == chunks - 1 and step == 0:
            return passed(c - 1, n - 3, 1) + 0.2 + 0.1 * side
        if c == chunks - 1 and step == n - 3 and side == 1:
            return begins(c - 1) + 0.1
        return 8.3 + c * lap + (2 * step + side) * 3.2

    def begins(c):
        return 10.5 + c * (lap + 2) + (2 * n - 3) * 3.2

    at(0.0, own_first, 0)
    at(0.1, swap_weights, 0)
    for to in ("core", "across", "beside"):
        at(0.2, own_block, "e", to)
    at(0.5, own_first, 1)
    at(5.0, own_second, 0)
    at(5.5, swap_weights, 1)
    at(5.6, swap_cotangent, 0)
    at(7.0, from_core, "e")
    at(7.1, turn, 0, 1)
    at(12.0, from_beside, "e", 0)
    at(13.5, from_across, "e")
    at(17.6, from_beside, "e", 1)
    for to in ("core", "across"):
        at(18.2, own_block, "l", to)
    at(19.0, turn, 2, 4)
    at(20.0, own_second, 1)
    for c in range(2, chunks):
        at(20.1 + (c - 2) * lap, swap_weights, c)
        at(21.9 + (c - 2) * lap, own_first, c)
        at(begins(c - 2) + 1.85, own_second, c, jnp.logical_not(inner))
        at(passed(c - 1, max(n - 3, 0), 1) + 0.1, own_second, c, inner)
    at(20.25, own_block, "l", "beside")
    for c in range(1, chunks):
        at(20.3, swap_cotangent, c)
    for c in range(chunks):
        for step in range(n - 1):
            for side in range(2):
                at(passed(c, step, side), pass_weights, c, step, side)
    at(begins(0) - 1.0, from_diagonal, "e")
    at(begins(0) - 1.7, third_block, "e")
    at(begins(0) - 1.65, fifth_block, "e")
    at(begins(0) - 1.6, turn, 3, 5)
    at(begins(0) - 0.75, turn, 6)
    at(begins(0) - 0.7, rest_blocks, "e")
    at(begins(0) - 0.6, turn, 7)
    at(30.0, from_core, "l")
    at(35.0, from_beside, "l", 0)
    at(37.0, from_across, "l")
    at(40.0, from_beside, "l", 1)
    at(begins(chunks - 2) + 2.9, third_block, "l")
    at(begins(chunks - 2) + 0.13, fifth_block, "l")
    at(begins(chunks - 2) + 3.4, from_diagonal, "l")
    at(begins(chunks - 2) + 4.0, rest_blocks, "l")
    corners = n - 1 - n // 2
    forwarded = passed(chunks - 1, max(n - 3, 0), 1)
    tail = begins(chunks - 1)
    more = (n - 4) * 5.6
    for c in range(chunks):
        final, middle_one = c == chunks - 1, c == chunks - 2
        start = begins(c)
        ahead = 1.1 if c == 0 else 0.0
        at(start - 0.2 - ahead, collect, c)
        at(start - 0.1 - ahead, got_cotangent, c)
        if c == 0:
            at(start - 0.05 - ahead, early, c, 0, tiles - 1)
            at(start, early, c, tiles - 1, tiles)
        elif final:
            for i, moment in ((3, 0.001), (1, 0.003), (2, 0.006), (0, 0.009)):
                at(tail + moment, early, c, i, i + 1)
        else:
            at(start, early, c)
        for i in range(n):
            for side in (1, 0):
                held = middle_one and i == n - 2 and side == 0
                moment = start + (1.8 if c == 0 else 0.2) + 0.1 * i
                if final:
                    order = 2 * i - side
                    moment = tail + (0.0096 - 0.0001 * side if i == 0 else 0.6 + 0.001 * order if i < n - 1 else 0.66)
                at(moment, weight_grads, c, i, side, not held)
                if held:
                    at(tail + 0.6 + 0.001 * (2 * i - 0.5), send_grads, c, i, side)
        first_sum = start + (7.0 if c == 0 else 10.5)
        for rank, side in enumerate((1, 0)):
            for step in range(n - 2):
                moment = first_sum + (2 * step + rank) * 2.7
                if c == 0 and step == n - 3 and rank == 1:
                    moment = max(moment, begins(1) + 0.15)
                if middle_one and step == n - 3:
                    moment = tail + 0.0025 + 0.004 * rank
                if final:
                    moment = tail + (0.65, 0.67, 0.705, 0.755)[min(2 * max(step - n + 4, 0) + rank, 3)] + 0.0001 * step
                at(moment, pass_sums, c, step, side, True)
            for step in range(corners):
                moment = first_sum + 4.0 + (2 * step + rank) * 2.8
                if final:
                    moment = tail + (0.71, 0.75)[rank] + 0.0001 * step
                elif middle_one:
                    moment = tail + 0.0085 + 0.05 * rank + 0.0001 * step
                else:
                    moment = max(moment, begins(chunks - 2) + 3.0 + 0.01 * rank + 0.0001 * step)
                at(moment, pass_sums, c, step, side, False)
        if final:
            at(tail + 0.80, settle, c, 1)
            at(tail + 0.85, settle, c, 0)
            at(tail + 0.89, finish, c)
        elif middle_one:
            at(tail + 0.655, settle, c, 1)
            at(tail + 0.845, settle, c, 0)
            at(tail + 0.87, finish, c)
        else:
            at(tail + 0.0047, settle, c, 1)
            at(tail + 0.58, settle, c, 0)
            at(tail + 0.68, finish, c)
        if not final:
            for i in range(tiles // 2):
                at(begins(chunks - 2) + (0.14 if i < tiles // 4 else 4.2) + 0.01 * c, late, c, 1, i)
                moment = tail + (0.76 if c == 0 else 0.801)
                if c == 0 and i < tiles // 4:
                    moment = begins(1) - 0.15
                at(moment, late, c, 0, i)
    for i in range(tiles):
        at(begins(chunks - 2) + (2.5 if i < tiles // 2 else 3.2) + 0.01 * i, input_grads, i)
    for i in range(tiles // 2):
        at(tail + (0.0046 if i == 0 else 0.0075), late, chunks - 1, 1, i)
        at(tail + (0.69 if i == 0 else 0.70), late, chunks - 1, 0, i)
    for q, made, summed in ((3, 0.002, 0.005), (1, 0.004, 0.008), (2, 0.007, 0.5), (0, 0.01, 0.665)):
        at(tail + made, input_pair, q)
        at(tail + summed, core_sum, q)
    at(tail + 0.63, turn_corner, 2)
    at(tail + 0.64, turn_corner, 0)
    at(tail + 0.708, turn_corner, 1)
    at(tail + 0.82, finish_input, 2)
    at(tail + 0.83, finish_input, 0)
    at(tail + 0.86, finish_input, 1)
    at(tail + 0.88, got_hidden)
    for _, _, action in sorted(plan, key=lambda entry: entry[:2]):
        action()
    copies.drain()
    local.drain()
    assert copies.total <= rsem.shape[0] and len(local.copies) <= lsem.shape[0]


def store_kernel(tp_count, hm, hr, gxv, g, hid, gx, og, ou, sem):
    tp, x = lax.axis_index("tp"), lax.rem(lax.axis_index("fs"), 2)
    tokens, half = gxv.shape[0], hm.shape[1]
    local = Locals(sem)
    for side in range(2):
        lane = pl.ds(pl.multiple_of((x if side == 0 else 1 - x) * half, LANES), half)
        for which, out in enumerate((og, ou)):
            local.start(("o", which, side), g.at[which, side], out.at[:, lane])
        for m in range(tp_count):
            src = (hm, hr)[side].at[pl.ds(m * tokens, tokens)]
            local.start(("h", side, m), src, hid.at[aligned(flips(tp, m) * tokens, tokens), lane])
    local.start("gx", gxv, gx)
    local.drain()


def local_part(fs_count, tp_count, x_late, x_early, d_hidden, w_gate, w_up, gate_sum, up_sum):
    n = fs_count // 2
    tokens, width = x_early.shape
    rows, cols = w_gate.shape
    half = cols // 2
    chunks = half // LANES
    group = tp_count * tokens
    pair = 2 * LANES
    remote = chunks * (4 * n + tp_count + 6) + 40
    locals_count = 4 * chunks + 2 + tp_count + 4
    any_spec = pl.BlockSpec(memory_space=pl.ANY)
    vmem_spec = pl.BlockSpec(memory_space=pltpu.VMEM)
    results = pl.pallas_call(
        functools.partial(layer_kernel, fs_count, tp_count),
        out_shape=(
            pltpu.VMEM((group, half), BF16),
            pltpu.VMEM((group, half), BF16),
            pltpu.VMEM(x_early.shape, BF16),
            pltpu.VMEM((2, 2, rows, half), F32),
        ),
        in_specs=[any_spec] * 7,
        out_specs=(vmem_spec,) * 4,
        scratch_shapes=[
            pltpu.VMEM((width, 2 * half), BF16),
            pltpu.VMEM((rows, 2 * half), BF16),
            pltpu.VMEM((2 * group, width), BF16),
            pltpu.VMEM((2 * group, width), BF16),
            pltpu.VMEM((width, 2 * group), BF16),
            pltpu.VMEM((2 * group, half), BF16),
            pltpu.VMEM((2 * group, 2 * half), BF16),
            pltpu.VMEM((width, 2 * half), BF16),
            pltpu.VMEM((2, width, 2 * half), BF16),
            pltpu.VMEM((2 * group, width), F32),
            pltpu.VMEM((2 * group, width), BF16),
            pltpu.VMEM((tp_count, tokens, width), BF16),
            pltpu.VMEM((6, tokens, width), BF16),
            pltpu.VMEM((group, half), BF16),
            pltpu.VMEM((chunks, rows, pair), BF16),
            pltpu.VMEM((chunks, rows, pair), BF16),
            pltpu.SemaphoreType.DMA((POOL,)),
            pltpu.SemaphoreType.DMA((remote,)),
            pltpu.SemaphoreType.DMA((locals_count,)),
        ],
        compiler_params=pltpu.CompilerParams(
            collective_id=0, has_side_effects=True, vmem_limit_bytes=58 * 1024 * 1024),
        name="layer",
    )(x_late, x_early, d_hidden, w_gate, w_up, gate_sum, up_sum)
    return pl.pallas_call(
        functools.partial(store_kernel, tp_count),
        out_shape=(
            jax.ShapeDtypeStruct((group, cols), BF16),
            jax.ShapeDtypeStruct(x_early.shape, BF16),
            jax.ShapeDtypeStruct(gate_sum.shape, F32),
            jax.ShapeDtypeStruct(up_sum.shape, F32),
        ),
        in_specs=[vmem_spec] * 4,
        out_specs=(any_spec,) * 4,
        scratch_shapes=[pltpu.SemaphoreType.DMA((2 * tp_count + 5,))],
        name="store",
    )(*(pltpu.with_memory_space_constraint(value, pltpu.VMEM) for value in results))


def solution(mesh):
    return jax.shard_map(
        functools.partial(local_part, mesh.shape["fs"], mesh.shape["tp"]),
        mesh=mesh,
        in_specs=(
            P(("fs", "tp"), None),
            P(("fs", "tp"), None),
            P("fs", "tp"),
            P("fs", "tp"),
            P("fs", "tp"),
            P("fs", "tp"),
            P("fs", "tp"),
        ),
        out_specs=(P("fs", "tp"), P(("fs", "tp"), None), P("fs", "tp"), P("fs", "tp")),
        check_vma=False,
    )
```

```python
import functools

import jax
import jax.numpy as jnp
from jax import lax
from jax.experimental import pallas as pl
from jax.experimental.pallas import tpu as pltpu
from jax.sharding import PartitionSpec as P

MESH = pl.DeviceIdType.MESH
F32 = jnp.float32
BF16 = jnp.bfloat16
LANES = 128
POOL = 48


def under(when, action):
    if when is None:
        action()
    else:
        pl.when(when)(action)


class Copies:
    def __init__(self, send_sem, recv_sem):
        self.send_sem, self.recv_sem = send_sem, recv_sem
        self.index, self.total, self.started, self.flying = {}, 0, 0, {}

    def number(self, key, count=1):
        if key not in self.index:
            self.index[key] = self.total
            self.total += count
        return self.index[key]

    def make(self, key, src, dst, device, send_at=0):
        at = self.number(key) if isinstance(key, tuple) else key
        return pltpu.make_async_remote_copy(
            src_ref=src, dst_ref=dst, send_sem=self.send_sem.at[send_at], recv_sem=self.recv_sem.at[at],
            device_id=device, device_id_type=MESH,
        )

    def start(self, key, src, dst, device, when=None):
        send_at = self.started % POOL
        self.settle(send_at)
        copy = self.make(key, src, dst, device, send_at)
        self.flying[send_at] = copy, when
        self.started += 1
        under(when, copy.start)

    def arrived(self, key, dst, device):
        self.make(key, dst, dst, device).wait_recv()

    def settle(self, send_at):
        if send_at in self.flying:
            copy, when = self.flying.pop(send_at)
            under(when, copy.wait_send)

    def drain(self):
        for send_at in sorted(self.flying):
            self.settle(send_at)


class Locals:
    def __init__(self, sem):
        self.sem, self.copies = sem, {}

    def start(self, key, src, dst, whole=None):
        if key not in self.copies:
            sem = self.sem.at[len(self.copies)]
            ref = dst if whole is None else whole
            self.copies[key] = [pltpu.make_async_copy(ref, ref, sem), False, sem]
        pltpu.make_async_copy(src, dst, self.copies[key][2]).start()

    def wait(self, key):
        entry = self.copies[key]
        if not entry[1]:
            entry[1] = True
            entry[0].wait()

    def drain(self):
        for key in self.copies:
            self.wait(key)


def flip(index, bit):
    return jnp.where(lax.rem(lax.div(index, bit), 2) == 0, index + bit, index - bit)


def flips(index, mask):
    for bit in (1, 2):
        if mask & bit:
            index = flip(index, bit)
    return index


def aligned(value, size):
    return pl.ds(pl.multiple_of(value, size), size)


NT = (((1,), (1,)), ((), ()))


def layer_kernel(
    fs_count, tp_count, xl, xe, dh, wg, wu, gs, us, hm, hr, gx, g,
    w, ws, te, tl, tt, ct, db, dw, rs, dxa, dxb, xk, xq, hs, fb, fr, ssem, rsem, lsem,
):
    fs, tp = lax.axis_index("fs"), lax.axis_index("tp")
    z, x = lax.div(fs, 2), lax.rem(fs, 2)
    n = fs_count // 2
    rows, cols = wg.shape
    tokens, width = xe.shape
    half = cols // 2
    chunks = half // LANES
    pair = 2 * LANES
    up = (jnp.minimum(z + 1, n - 1) * 2 + x, tp)
    down = (jnp.maximum(z - 1, 0) * 2 + x, tp)
    beside = (z * 2 + 1 - x, tp)
    across = (fs, flip(tp, 2))
    core = (fs, flip(tp, 1))
    far = {"core": core, "across": across, "beside": beside}
    copies, local = Copies(ssem, rsem), Locals(lsem)

    def cc(c):
        return pl.ds(c * pair, pair)

    def wrows(at, side):
        return aligned((at * 2 + side) * rows, rows)

    def slot(r):
        return pl.ds(r * tokens, tokens)

    barrier = pltpu.get_barrier_semaphore()

    def greet(device):
        pl.semaphore_signal(barrier, inc=1, device_id=device, device_id_type=MESH)

    pl.when(z < n - 1)(lambda: greet(up))
    pl.when(z > 0)(lambda: greet(down))
    for device in far.values():
        greet(device)
    for c in range(chunks):
        for name, src, at in (("g", wg, 0), ("u", wu, LANES)):
            lane = pl.ds(c * pair + at, LANES)
            local.start(("w", c), src.at[:, aligned(x * half + c * LANES, LANES)], w.at[wrows(z, x), lane], w.at[wrows(z, x), cc(c)])
            local.start(("ws", c), src.at[:, aligned((1 - x) * half + c * LANES, LANES)], ws.at[:, lane], ws.at[:, cc(c)])
        if c == 0:
            local.start("te", xe, te.at[slot(0)])
    local.start("tl", xl, tl.at[slot(0)])
    for m in range(tp_count):
        src = dh.at[aligned(flips(tp, m) * tokens, tokens), pl.ds(pl.multiple_of(x * half, LANES), half)]
        local.start("ct", src, ct.at[slot(m)], ct.at[pl.ds(0, tp_count * tokens)])
    for side in range(2):
        lane = pl.ds(pl.multiple_of((x if side == 0 else 1 - x) * half, LANES), half)
        for which, src in enumerate((gs, us)):
            local.start(("g", side), src.at[:, lane], g.at[which, side], g.at[:, side])

    ends = jnp.where(z < n - 1, 1, 0) + jnp.where(z > 0, 1, 0)
    pl.semaphore_wait(barrier, len(far) + ends)

    plan = []

    def at(time, action, *args):
        plan.append((time, len(plan), functools.partial(action, *args)))

    ways = (("u", up, z < n - 1), ("d", down, z > 0))

    def own_first(c):
        local.wait(("w", c))
        ref = w.at[wrows(z, x), cc(c)]
        for name, device, when in ways:
            copies.start(copies.number(("w", c, 0), n) + z, ref, ref, device, when)

    def swap_weights(c):
        local.wait(("ws", c))
        copies.start(("b", c), ws.at[:, cc(c)], w.at[wrows(z, x), cc(c)], beside)

    inner = (z > 0) & (z < n - 1)

    def own_second(c, where=None):
        def action():
            copies.arrived(("b", c), ref, beside)

        ref = w.at[wrows(z, 1 - x), cc(c)]
        under(where, action)
        for name, device, when in ways:
            copies.start(copies.number(("w", c, 1), n) + z, ref, ref, device, when if where is None else when & where)

    def weight_piece(c, step, side, name):
        origin = z - 1 - step if name == "u" else z + 1 + step
        has = origin >= 0 if name == "u" else origin <= n - 1
        origin = jnp.clip(origin, 0, n - 1)
        return w.at[wrows(origin, x if side == 0 else 1 - x), cc(c)], has, copies.number(("w", c, side), n) + origin

    def pass_weights(c, step, side):
        if step == n - 2:
            return
        for name, device, when in ways:
            ref, has, key = weight_piece(c, step, side, name)
            pl.when(has & when)(lambda: copies.arrived(key, ref, device))
            copies.start(key, ref, ref, device, has & when)

    def collect(c):
        for step in range(n - 1):
            for side in range(2):
                for name, device, when in ways:
                    ref, has, key = weight_piece(c, step, side, name)
                    if step < n - 2:
                        has = has & jnp.logical_not(when)
                    pl.when(has)(lambda: copies.arrived(key, ref, device))

    arrays = {"e": (te, xe, "te"), "l": (tl, xl, "tl")}

    def block(kind, r, part):
        first, size = (0, tokens) if part is None else part
        return arrays[kind][0].at[pl.ds(r * tokens + first, size)]

    def send_block(kind, to, src, dst, part=None):
        copies.start((kind, to, dst, None if to == "core" else part), block(kind, src, part), block(kind, dst, part), far[to])

    def got_block(kind, to, dst, part=None):
        copies.arrived((kind, to, dst, part), block(kind, dst, part), far[to])

    middle = tokens // 2
    halves = ((0, middle), (middle, middle))
    side_way = {"e": tokens // 8, "l": 0}
    last_part = {kind: (tokens - size, size) for kind, size in side_way.items()}
    corner = {kind: (halves[0], (middle, middle - size)) for kind, size in side_way.items()}

    def own_block(kind, to):
        local.wait(arrays[kind][2])
        dst = {"core": 1, "across": 2, "beside": 4}[to]
        for part in halves if to == "beside" else (None,):
            send_block(kind, to, 0, dst, part)

    def from_core(kind):
        got_block(kind, "core", 1)

    def from_across(kind):
        got_block(kind, "across", 2)
        if side_way[kind]:
            send_block(kind, "beside", 2, 6, last_part[kind])
        send_block(kind, "core", 2, 3)

    def from_beside(kind, half_at):
        got_block(kind, "beside", 4, halves[half_at])
        send_block(kind, "across", 4, 6, corner[kind][half_at])
        send_block(kind, "core", 4, 5, halves[half_at])

    def from_diagonal(kind):
        for part in corner[kind]:
            got_block(kind, "across", 6, part)
            send_block(kind, "core", 6, 7, part)
        if side_way[kind]:
            got_block(kind, "beside", 6, last_part[kind])
            send_block(kind, "core", 6, 7, last_part[kind])

    def third_block(kind):
        got_block(kind, "core", 3)

    def fifth_block(kind):
        got_block(kind, "core", 5)

    def rest_blocks(kind):
        got_block(kind, "core", 7)

    def turn(*blocks):
        for r in blocks:
            tt[:, slot(r)] = te[slot(r), :].T

    def swap_cotangent(c):
        lane = aligned((1 - x) * half + c * LANES, LANES)
        for m in range(tp_count):
            src = dh.at[aligned(flips(tp, m) * tokens, tokens), lane]
            dst = ct.at[slot(tp_count + m), pl.ds(c * LANES, LANES)]
            copies.start(("c", c), src, dst, beside)

    def got_cotangent(c):
        local.wait("ct")
        theirs = pl.ds(tp_count * tokens, tp_count * tokens)
        copies.arrived(("c", c), ct.at[theirs, pl.ds(c * LANES, LANES)], beside)

    tile = 2 * tokens
    tiles = 2 * tp_count * tokens // tile

    def early(c, low=0, high=tiles):
        def body(i, carry):
            at_rows = aligned(i * tile, tile)
            pre = jnp.dot(te[at_rows, :], w[:, cc(c)], preferred_element_type=F32)
            gate, up_part = pre[:, :LANES], pre[:, LANES:]
            s = jax.nn.sigmoid(gate)
            cot = ct[at_rows, pl.ds(c * LANES, LANES)].astype(F32)
            db[at_rows, pl.ds(c * pair, LANES)] = (cot * up_part * s * (1.0 + gate * (1.0 - s))).astype(BF16)
            db[at_rows, pl.ds(c * pair + LANES, LANES)] = (cot * gate * s).astype(BF16)
            return carry

        lax.fori_loop(low, high, body, 0, unroll=2 if (high - low) % 2 == 0 else 1)

    def late(c, first, i):
        out = hs if first else hm
        lane = pl.ds(c * LANES, LANES)

        def body(at_tile, carry):
            at_rows = aligned(at_tile * tile, tile)
            from_rows = aligned((first * tiles // 2 + at_tile) * tile, tile)
            pre = jnp.dot(tl[from_rows, :], w[:, cc(c)], preferred_element_type=F32)
            gate, up_part = pre[:, :LANES], pre[:, LANES:]
            out[at_rows, lane] = (gate * jax.nn.sigmoid(gate) * up_part).astype(BF16)
            return carry

        lax.fori_loop(i, i + 1, body, 0)
        if first:
            at_rows = pl.ds(i * tile, tile)
            copies.start(("h", c), hs.at[at_rows, lane], hr.at[at_rows, lane], beside)

    def got_hidden():
        for c in range(chunks):
            copies.arrived(("h", c), hr.at[:, pl.ds(c * LANES, LANES)], beside)

    def sum_key(c, side, d, target, receiver):
        base = copies.number(("r", c, side), n + 1)
        return base + jnp.where((d == 1) & (target == receiver), n, target)

    def beyond(d, target):
        return jnp.where(d == 0, target - z, z - target) > 0

    def onward(d):
        to = jnp.clip(jnp.where(d == 0, z + 1, z - 1), 0, n - 1)
        return to, (to * 2 + x, tp)

    def srows(target, side):
        return wrows(target, x if side == 0 else 1 - x)

    def trows(target):
        return aligned(target * 2 * rows, 2 * rows)

    def grad_target(i):
        return jnp.where(z < n // 2, n - 1 - i, i)

    def weight_grads(c, i, side, send=True):
        piece = srows(grad_target(i), side)
        dw[piece, cc(c)] = jnp.dot(tt[piece, :], db[:, cc(c)], preferred_element_type=F32).astype(BF16)
        if send:
            send_grads(c, i, side)

    def send_grads(c, i, side):
        target = grad_target(i)
        piece = srows(target, side)
        d = jnp.where(z == 0, 0, 1)
        to, device = onward(d)
        when = jnp.logical_not(inner) & beyond(d, target)
        copies.start(sum_key(c, side, d, target, to), dw.at[piece, cc(c)], rs.at[d, piece, cc(c)], device, when)

    def add(a, b):
        return (a.astype(F32) + b.astype(F32)).astype(BF16)

    def pass_sums(c, step, side, near):
        d = jnp.where(z < n // 2, 0, 1) if near else jnp.where(z < n // 2, 1, 0)
        target = jnp.where(d == 0, n - 1 - step, step)
        passes = inner & beyond(d, target)
        to, device = onward(d)
        ref = rs.at[d, srows(target, side), cc(c)]
        own = dw.at[srows(target, side), cc(c)]

        def action():
            copies.arrived(sum_key(c, side, d, target, z), ref, device)
            ref[...] = add(ref[...], own[...])

        pl.when(passes)(action)
        copies.start(sum_key(c, side, d, target, to), ref, ref, device, passes)

    def settle(c, side):
        rows_here = srows(z, side)
        for d, behind in ((0, z > 0), (1, z < n - 1)):
            ref = rs.at[d, rows_here, cc(c)]

            def take():
                copies.arrived(sum_key(c, side, d, z, z), ref, beside)

            def blank():
                ref[...] = jnp.zeros((rows, pair), BF16)

            pl.when(behind)(take)
            pl.when(jnp.logical_not(behind))(blank)
        total = dw[rows_here, cc(c)].astype(F32)
        for d in range(2):
            total = total + rs[d, rows_here, cc(c)].astype(F32)
        if side == 1:
            fb[c] = total.astype(BF16)
            copies.start(("f", c), fb.at[c], fr.at[c], beside)
            return
        lane = pl.ds(c * LANES, LANES)
        for which in range(2):
            local.wait(("g", 0))
            g[which, 0, :, lane] = g[which, 0, :, lane] + total[:, which * LANES : (which + 1) * LANES]

    def finish(c):
        copies.arrived(("f", c), fr.at[c], beside)
        lane = pl.ds(c * LANES, LANES)
        for which in range(2):
            local.wait(("g", 1))
            g[which, 1, :, lane] = g[which, 1, :, lane] + fr[c, :, pl.ds(which * LANES, LANES)].astype(F32)

    depth = (chunks - 1) * pair
    bands = [pl.ds(i * (width // 4), width // 4) for i in range(4)]

    def input_grads(i):
        at_rows = pl.ds(i * tile, tile)
        for band in bands:
            dxa[at_rows, band] = lax.dot_general(
                db[at_rows, pl.ds(0, depth)], w[band, pl.ds(0, depth)], NT, preferred_element_type=F32)

    end = pl.ds(depth, pair)

    def input_pair(q):
        at_rows = pl.ds(q * tile, tile)
        for band in bands:
            value = lax.dot_general(db[at_rows, end], w[band, end], NT, preferred_element_type=F32)
            dxb[at_rows, band] = (dxa[at_rows, band] + value).astype(BF16)
        copies.start(("k", q), dxb.at[slot(2 * q + 1)], xk.at[q], core)

    unit = width // 16
    parts = (pl.ds(0, 7 * unit), pl.ds(7 * unit, 7 * unit), pl.ds(14 * unit, 2 * unit))
    routes = {
        3: (("y", 0, 0), ("y", 0, 1), ("x", 2, 2)),
        1: (("y", 1, 0), ("y", 1, 1)),
        2: (("x", 3, 2),),
        0: (),
    }

    def core_sum(q):
        copies.arrived(("k", q), xk.at[q], core)
        xk[q] = add(xk[q], dxb[slot(2 * q), :])
        for name, place, at_part in routes[q]:
            part = parts[at_part]
            device = across if name == "y" else beside
            copies.start(("q", place, at_part), xk.at[q, :, part], xq.at[place, :, part], device)

    def turn_corner(at_part):
        place, q, to, device = (2, 1, 5, across) if at_part == 2 else (0, 2, 4, beside)
        part = parts[at_part]
        copies.arrived(("q", place, at_part), xq.at[place, :, part], device)
        xq[place, :, part] = add(xq[place, :, part], xk[q, :, part])
        copies.start(("q", to, at_part), xq.at[place, :, part], xq.at[to, :, part], device)

    def finish_input(at_part):
        part = parts[at_part]
        total = xk[0, :, part].astype(F32)
        for place in (3, 5) if at_part == 2 else (1, 4):
            copies.arrived(("q", place, at_part), xq.at[place, :, part], core)
            total = total + xq[place, :, part].astype(F32)
        gx[:, part] = total.astype(BF16)

    lap = 13.5 + (n - 4) * 6.4

    def passed(c, step, side):
        if c == 0 and step == 0 and side == 0:
            return 6.5
        if c == 1 and step == 0 and side == 1:
            return begins(0) + 0.05
        if c == 1 and step == 1 and side == 0:
            return begins(0) + 0.2
        if c == chunks - 1 and step == 0:
            return passed(c - 1, n - 3, 1) + 0.2 + 0.1 * side
        if c == chunks - 1 and step == n - 3 and side == 1:
            return begins(c - 1) + 0.1
        return 8.3 + c * lap + (2 * step + side) * 3.2

    def begins(c):
        return 10.5 + c * (lap + 2) + (2 * n - 3) * 3.2

    at(0.0, own_first, 0)
    at(0.1, swap_weights, 0)
    for to in ("core", "across", "beside"):
        at(0.2, own_block, "e", to)
    at(0.5, own_first, 1)
    at(5.0, own_second, 0)
    at(5.5, swap_weights, 1)
    at(5.6, swap_cotangent, 0)
    at(7.0, from_core, "e")
    at(7.1, turn, 0, 1)
    at(12.0, from_beside, "e", 0)
    at(13.5, from_across, "e")
    at(17.6, from_beside, "e", 1)
    for to in ("core", "across"):
        at(18.2, own_block, "l", to)
    at(19.0, turn, 2, 4)
    at(20.0, own_second, 1)
    for c in range(2, chunks):
        at(20.1 + (c - 2) * lap, swap_weights, c)
        at(21.9 + (c - 2) * lap, own_first, c)
        at(begins(c - 2) + 1.85, own_second, c, jnp.logical_not(inner))
        at(passed(c - 1, max(n - 3, 0), 1) + 0.1, own_second, c, inner)
    at(20.25, own_block, "l", "beside")
    for c in range(1, chunks):
        at(20.3, swap_cotangent, c)
    for c in range(chunks):
        for step in range(n - 1):
            for side in range(2):
                at(passed(c, step, side), pass_weights, c, step, side)
    at(begins(0) - 1.0, from_diagonal, "e")
    at(begins(0) - 1.7, third_block, "e")
    at(begins(0) - 1.65, fifth_block, "e")
    at(begins(0) - 1.6, turn, 3, 5)
    at(begins(0) - 0.75, turn, 6)
    at(begins(0) - 0.7, rest_blocks, "e")
    at(begins(0) - 0.6, turn, 7)
    at(30.0, from_core, "l")
    at(35.0, from_beside, "l", 0)
    at(37.0, from_across, "l")
    at(40.0, from_beside, "l", 1)
    at(begins(chunks - 2) + 2.9, third_block, "l")
    at(begins(chunks - 2) + 0.13, fifth_block, "l")
    at(begins(chunks - 2) + 3.4, from_diagonal, "l")
    at(begins(chunks - 2) + 4.0, rest_blocks, "l")
    corners = n - 1 - n // 2
    forwarded = passed(chunks - 1, max(n - 3, 0), 1)
    tail = begins(chunks - 1)
    more = (n - 4) * 5.6
    for c in range(chunks):
        final, middle_one = c == chunks - 1, c == chunks - 2
        start = begins(c)
        ahead = 1.1 if c == 0 else 0.0
        at(start - 0.2 - ahead, collect, c)
        at(start - 0.1 - ahead, got_cotangent, c)
        if c == 0:
            at(start - 0.05 - ahead, early, c, 0, tiles - 1)
            at(start, early, c, tiles - 1, tiles)
        elif final:
            for i, moment in ((3, 0.001), (1, 0.003), (2, 0.006), (0, 0.009)):
                at(tail + moment, early, c, i, i + 1)
        else:
            at(start, early, c)
        for i in range(n):
            for side in (1, 0):
                held = middle_one and i == n - 2 and side == 0
                moment = start + (1.8 if c == 0 else 0.2) + 0.1 * i
                if final:
                    order = 2 * i - side
                    moment = tail + (0.0096 - 0.0001 * side if i == 0 else 0.6 + 0.001 * order if i < n - 1 else 0.66)
                at(moment, weight_grads, c, i, side, not held)
                if held:
                    at(tail + 0.6 + 0.001 * (2 * i - 0.5), send_grads, c, i, side)
        first_sum = start + (7.0 if c == 0 else 10.5)
        for rank, side in enumerate((1, 0)):
            for step in range(n - 2):
                moment = first_sum + (2 * step + rank) * 2.7
                if c == 0 and step == n - 3 and rank == 1:
                    moment = max(moment, begins(1) + 0.15)
                if middle_one and step == n - 3:
                    moment = tail + 0.0025 + 0.004 * rank
                if final:
                    moment = tail + (0.65, 0.67, 0.705, 0.755)[min(2 * max(step - n + 4, 0) + rank, 3)] + 0.0001 * step
                at(moment, pass_sums, c, step, side, True)
            for step in range(corners):
                moment = first_sum + 4.0 + (2 * step + rank) * 2.8
                if final:
                    moment = tail + (0.71, 0.75)[rank] + 0.0001 * step
                elif middle_one:
                    moment = tail + 0.0085 + 0.05 * rank + 0.0001 * step
                else:
                    moment = max(moment, begins(chunks - 2) + 3.0 + 0.01 * rank + 0.0001 * step)
                at(moment, pass_sums, c, step, side, False)
        if final:
            at(tail + 0.80, settle, c, 1)
            at(tail + 0.85, settle, c, 0)
            at(tail + 0.89, finish, c)
        elif middle_one:
            at(tail + 0.655, settle, c, 1)
            at(tail + 0.845, settle, c, 0)
            at(tail + 0.87, finish, c)
        else:
            at(tail + 0.0047, settle, c, 1)
            at(tail + 0.58, settle, c, 0)
            at(tail + 0.68, finish, c)
        if not final:
            for i in range(tiles // 2):
                at(begins(chunks - 2) + (0.14 if i < tiles // 4 else 4.2) + 0.01 * c, late, c, 1, i)
                moment = tail + (0.76 if c == 0 else 0.801)
                if c == 0 and i < tiles // 4:
                    moment = begins(1) - 0.15
                at(moment, late, c, 0, i)
    for i in range(tiles):
        at(begins(chunks - 2) + (2.5 if i < tiles // 2 else 3.2) + 0.01 * i, input_grads, i)
    for i in range(tiles // 2):
        at(tail + (0.0046 if i == 0 else 0.0075), late, chunks - 1, 1, i)
        at(tail + (0.69 if i == 0 else 0.70), late, chunks - 1, 0, i)
    for q, made, summed in ((3, 0.002, 0.005), (1, 0.004, 0.008), (2, 0.007, 0.5), (0, 0.01, 0.665)):
        at(tail + made, input_pair, q)
        at(tail + summed, core_sum, q)
    at(tail + 0.63, turn_corner, 2)
    at(tail + 0.64, turn_corner, 0)
    at(tail + 0.708, turn_corner, 1)
    at(tail + 0.82, finish_input, 2)
    at(tail + 0.83, finish_input, 0)
    at(tail + 0.86, finish_input, 1)
    at(tail + 0.88, got_hidden)
    for _, _, action in sorted(plan, key=lambda entry: entry[:2]):
        action()
    copies.drain()
    local.drain()
    assert copies.total <= rsem.shape[0] and len(local.copies) <= lsem.shape[0]


def store_kernel(tp_count, hm, hr, gxv, g, hid, gx, og, ou, sem):
    tp, x = lax.axis_index("tp"), lax.rem(lax.axis_index("fs"), 2)
    tokens, half = gxv.shape[0], hm.shape[1]
    local = Locals(sem)
    for side in range(2):
        lane = pl.ds(pl.multiple_of((x if side == 0 else 1 - x) * half, LANES), half)
        for which, out in enumerate((og, ou)):
            local.start(("o", which, side), g.at[which, side], out.at[:, lane])
        for m in range(tp_count):
            src = (hm, hr)[side].at[pl.ds(m * tokens, tokens)]
            local.start(("h", side, m), src, hid.at[aligned(flips(tp, m) * tokens, tokens), lane])
    local.start("gx", gxv, gx)
    local.drain()


def local_part(fs_count, tp_count, x_late, x_early, d_hidden, w_gate, w_up, gate_sum, up_sum):
    n = fs_count // 2
    tokens, width = x_early.shape
    rows, cols = w_gate.shape
    half = cols // 2
    chunks = half // LANES
    group = tp_count * tokens
    pair = 2 * LANES
    remote = chunks * (4 * n + 6) + tp_count + 28
    locals_count = 2 * chunks + 5
    any_spec = pl.BlockSpec(memory_space=pl.ANY)
    vmem_spec = pl.BlockSpec(memory_space=pltpu.VMEM)
    results = pl.pallas_call(
        functools.partial(layer_kernel, fs_count, tp_count),
        out_shape=(
            pltpu.VMEM((group, half), BF16),
            pltpu.VMEM((group, half), BF16),
            pltpu.VMEM(x_early.shape, BF16),
            pltpu.VMEM((2, 2, rows, half), F32),
        ),
        in_specs=[any_spec] * 7,
        out_specs=(vmem_spec,) * 4,
        scratch_shapes=[
            pltpu.VMEM((width, 2 * half), BF16),
            pltpu.VMEM((rows, 2 * half), BF16),
            pltpu.VMEM((2 * group, width), BF16),
            pltpu.VMEM((2 * group, width), BF16),
            pltpu.VMEM((width, 2 * group), BF16),
            pltpu.VMEM((2 * group, half), BF16),
            pltpu.VMEM((2 * group, 2 * half), BF16),
            pltpu.VMEM((width, 2 * half), BF16),
            pltpu.VMEM((2, width, 2 * half), BF16),
            pltpu.VMEM((2 * group, width), F32),
            pltpu.VMEM((2 * group, width), BF16),
            pltpu.VMEM((tp_count, tokens, width), BF16),
            pltpu.VMEM((6, tokens, width), BF16),
            pltpu.VMEM((group, half), BF16),
            pltpu.VMEM((chunks, rows, pair), BF16),
            pltpu.VMEM((chunks, rows, pair), BF16),
            pltpu.SemaphoreType.DMA((POOL,)),
            pltpu.SemaphoreType.DMA((remote,)),
            pltpu.SemaphoreType.DMA((locals_count,)),
        ],
        compiler_params=pltpu.CompilerParams(
            collective_id=0, has_side_effects=True, vmem_limit_bytes=58 * 1024 * 1024),
        name="layer",
    )(x_late, x_early, d_hidden, w_gate, w_up, gate_sum, up_sum)
    return pl.pallas_call(
        functools.partial(store_kernel, tp_count),
        out_shape=(
            jax.ShapeDtypeStruct((group, cols), BF16),
            jax.ShapeDtypeStruct(x_early.shape, BF16),
            jax.ShapeDtypeStruct(gate_sum.shape, F32),
            jax.ShapeDtypeStruct(up_sum.shape, F32),
        ),
        in_specs=[vmem_spec] * 4,
        out_specs=(any_spec,) * 4,
        scratch_shapes=[pltpu.SemaphoreType.DMA((2 * tp_count + 5,))],
        name="store",
    )(*(pltpu.with_memory_space_constraint(value, pltpu.VMEM) for value in results))


def solution(mesh):
    return jax.shard_map(
        functools.partial(local_part, mesh.shape["fs"], mesh.shape["tp"]),
        mesh=mesh,
        in_specs=(
            P(("fs", "tp"), None),
            P(("fs", "tp"), None),
            P("fs", "tp"),
            P("fs", "tp"),
            P("fs", "tp"),
            P("fs", "tp"),
            P("fs", "tp"),
        ),
        out_specs=(P("fs", "tp"), P(("fs", "tp"), None), P("fs", "tp"), P("fs", "tp")),
        check_vma=False,
    )
```
